32 devices in a mesh: dp: 4 (over y, x), kv: 4 (over z), tp: 2 (over core).
Axes of the slice: x: 2, y: 2, z: 4, core: 2. Of those that a mesh axis runs over, the one named last changes fastest.
Arguments:
- tokens: bfloat16 [4, 3072, 2048], P('dp', 'kv'), may hold values from -60 to 60
- query_weight: bfloat16 [2048, 1024], P(None, 'tp'), may hold values from -0.125 to 0.125
- key_weight: bfloat16 [2048, 256], P(None, 'tp'), may hold values from -0.125 to 0.125
- value_weight: bfloat16 [2048, 256], P(None, 'tp'), may hold values from -0.125 to 0.125
- out_weight: bfloat16 [1024, 2048], P('tp'), may hold values from -3 to 3
- norm_gain: float32 [2048], P('tp'), may hold values from 0.1 to 1.9
- chosen_owner: int32 [4, 24, 4], P('dp'), may hold values from -1 to 3, as said below
- chosen_part: int32 [4, 24, 4], P('dp'), may hold values from 0 to 11, as said below
Outputs:
- attended: bfloat16 [4, 3072, 2048], P('dp', 'kv', 'tp')
The draws below stay inside these ranges and needn't reach their ends.
Inputs may be any that keep to these rules, and one draw needn't show every extreme that they name: `chosen_owner`: within a row the indices other than -1 are different. Every named key block lies wholly before its query block's first position. Among the 6 rows of one index of kv, no index is named by more than 6 rows. `chosen_part`: 0 where the owner is -1.
All inputs are finite; a program needn't handle non-finite values.
Results may differ from the reference program's by a relative error of at most 0.014.
The reference program's roundings to bfloat16 on the way count: a program that leaves them out, or rounds other values in their place, can miss the bound.
Values may be sent and summed in bfloat16 or wider, within the bound.
A program may use at most 128 MiB of HBM per device.

```python
import jax
import jax.numpy as jnp
from jax import lax

D = 2048
HEADS = 16
KV_HEADS = 4
HEAD_DIM = 64
QUERY_BLOCK = 128
KEY_BLOCK = 64
SEQS = 4
SEQ = 3072
QBLOCKS = 24
QBLOCKS_DEV = 6
KBLOCKS_DEV = 12
CHOSEN = 4
N_KV = 4
N_TP = 2


def draw_tokens(key, part):
    base = jax.random.normal(jax.random.fold_in(key, 11), (SEQS, SEQ, D), jnp.float32)
    base = jnp.clip(base, -6.0, 6.0)
    return base.astype(jnp.bfloat16)


def draw_out_weight(key, part):
    base = jax.random.normal(jax.random.fold_in(key, 21), (HEADS * HEAD_DIM, D), jnp.float32)
    base = jnp.clip(base, -6.0, 6.0) * (HEADS * HEAD_DIM) ** (-0.5)
    column = jnp.arange(D, dtype=jnp.float32) / D
    jitter = jnp.exp(jax.random.uniform(jax.random.fold_in(key, 22), (D,), jnp.float32, -0.5, 0.5))
    rising = 3.0 ** column
    return (base * (rising * jitter)[None, :] * 0.5).astype(jnp.bfloat16)


def chosen_pair(key):
    block_ids = jnp.arange(QBLOCKS, dtype=jnp.int32)
    device_ids = block_ids // QBLOCKS_DEV
    local_ids = block_ids % QBLOCKS_DEV
    owners = jnp.arange(N_KV, dtype=jnp.int32)
    earlier = owners[None, :] < device_ids[:, None]
    itself = jnp.logical_and(owners[None, :] == device_ids[:, None], local_ids[:, None] > 0)
    allowed = jnp.logical_or(earlier, itself)
    forced = jnp.logical_or(jnp.logical_or(owners[None, :] == 0, owners[None, :] == device_ids[:, None] - 1), jnp.logical_or(owners[None, :] == device_ids[:, None] - N_KV // 2, owners[None, :] == device_ids[:, None]))
    forced = jnp.logical_and(forced, allowed)
    noise = jax.random.randint(jax.random.fold_in(key, 31), (SEQS, QBLOCKS, N_KV), 0, 16384)
    scores = noise + (N_KV - owners)[None, None, :] * (16384 // N_KV) + forced[None].astype(jnp.int32) * 1048576
    scores = jnp.where(allowed[None], scores, -2097152)
    scores = scores * 64 + owners[None, None, :]
    picked = lax.top_k(scores, CHOSEN)[1].astype(jnp.int32)
    valid = jnp.take_along_axis(jnp.broadcast_to(allowed[None], (SEQS, QBLOCKS, N_KV)), picked, axis=2)
    owner_out = jnp.where(valid, picked, -1).astype(jnp.int32)
    limit = jnp.where(picked == device_ids[None, :, None], QUERY_BLOCK // KEY_BLOCK * local_ids[None, :, None], KBLOCKS_DEV)
    limit = jnp.maximum(limit, 1)
    raw_part = jax.random.randint(jax.random.fold_in(key, 32), (SEQS, QBLOCKS, CHOSEN), 0, 1048576)
    part_out = jnp.where(valid, raw_part % limit, 0).astype(jnp.int32)
    return (owner_out, part_out)


def draw_chosen_owner(key, part):
    return chosen_pair(jax.random.fold_in(key, 41))[0]


def draw_chosen_part(key, part):
    return chosen_pair(jax.random.fold_in(key, 41))[1]


def level_of(own_key, dims, cuts, least, high):
    gain, own = 1.0, jax.random.fold_in(own_key, 6)
    for axis_at, parts in cuts:
        draws = jnp.exp(jax.random.uniform(jax.random.fold_in(own, axis_at), (parts,), jnp.float32, least / len(cuts), high / len(cuts)))
        gain = gain * jnp.repeat(draws, dims[axis_at] // parts).reshape([-1 if axis == axis_at else 1 for axis in range(len(dims))])
    return gain


def bell_draw(rng, shape, deviation, bound, split=(), held_as=jnp.bfloat16):
    factor_of = level_of(rng, shape, split, -0.22, 0.18) if split else 1.0
    drawn = jax.random.normal(rng, shape, jnp.float32) * deviation * factor_of
    return jnp.minimum(jnp.maximum(drawn, -bound), bound).astype(held_as)


def setup_inputs(seed: int = 0) -> dict:
    keys = jax.random.split(jax.random.key(seed), 9)
    tokens = draw_tokens(jax.random.fold_in(keys[8], 71), 0)
    query_weight = bell_draw(keys[1], (D, HEADS * HEAD_DIM), D ** -0.5, 0.125, ((1, 2),))
    key_weight = bell_draw(keys[2], (D, KV_HEADS * HEAD_DIM), D ** -0.5, 0.125, ((1, 2),))
    value_weight = bell_draw(keys[3], (D, KV_HEADS * HEAD_DIM), D ** -0.5, 0.125, ((1, 2),))
    out_weight = draw_out_weight(jax.random.fold_in(keys[8], 71), 0)
    norm_gain = jnp.clip(1.0 + 0.18 * jax.random.normal(keys[5], (D,), jnp.float32), 0.1, 1.9)
    chosen_owner = draw_chosen_owner(jax.random.fold_in(keys[8], 71), 0)
    chosen_part = draw_chosen_part(jax.random.fold_in(keys[8], 71), 0)
    return {"tokens": tokens, "query_weight": query_weight, "key_weight": key_weight, "value_weight": value_weight, "out_weight": out_weight, "norm_gain": norm_gain, "chosen_owner": chosen_owner, "chosen_part": chosen_part}


rope_base = 10000.0
norm_eps = 1e-06

def rotate(head_rows, positions):
    half_dim = head_rows.shape[-1] // 2
    frequency = rope_base ** (-jnp.arange(half_dim, dtype=jnp.float32) / half_dim)
    angles = positions.astype(jnp.float32)[:, None] * frequency
    cosine = jnp.cos(angles)[:, None, :]
    sine_part = jnp.sin(angles)[:, None, :]
    first_half = head_rows[..., :half_dim]
    second_half = head_rows[..., half_dim:]
    return jnp.concatenate([first_half * cosine - second_half * sine_part, second_half * cosine + first_half * sine_part], axis=-1)

def reference(tokens, query_weight, key_weight, value_weight, out_weight, norm_gain, chosen_owner, chosen_part):
    group_size = HEADS // KV_HEADS
    lower_mask = jnp.arange(QUERY_BLOCK)[:, None] >= jnp.arange(QUERY_BLOCK)[None, :]

    def one_sequence(seq_items):
        row_data, owner_ids, part_ids = seq_items
        positions = jnp.arange(SEQ, dtype=jnp.int32)
        queries = rotate(jnp.dot(row_data, query_weight, preferred_element_type=jnp.float32).reshape(SEQ, HEADS, HEAD_DIM), positions).astype(jnp.bfloat16)
        key_rows = rotate(jnp.dot(row_data, key_weight, preferred_element_type=jnp.float32).reshape(SEQ, KV_HEADS, HEAD_DIM), positions).astype(jnp.bfloat16)
        value_rows = jnp.dot(row_data, value_weight, preferred_element_type=jnp.float32).astype(jnp.bfloat16).reshape(SEQ, KV_HEADS, HEAD_DIM)
        key_blocks = key_rows.reshape(SEQ // KEY_BLOCK, KEY_BLOCK, KV_HEADS, HEAD_DIM)
        value_blocks = value_rows.reshape(SEQ // KEY_BLOCK, KEY_BLOCK, KV_HEADS, HEAD_DIM)
        slot_valid = owner_ids >= 0
        chosen_ids = jnp.where(slot_valid, owner_ids * KBLOCKS_DEV + part_ids, 0).astype(jnp.int32)

        def one_block(block_index):
            block_start = (block_index * QUERY_BLOCK).astype(jnp.int32)
            picked_ids = chosen_ids[block_index]
            valid_row = slot_valid[block_index]
            block_queries = lax.dynamic_slice_in_dim(queries, block_start, QUERY_BLOCK, 0).reshape(QUERY_BLOCK, KV_HEADS, group_size, HEAD_DIM).astype(jnp.float32)
            own_keys = lax.dynamic_slice_in_dim(key_rows, block_start, QUERY_BLOCK, 0)
            own_values = lax.dynamic_slice_in_dim(value_rows, block_start, QUERY_BLOCK, 0)
            chosen_keys = key_blocks[picked_ids].reshape(CHOSEN * KEY_BLOCK, KV_HEADS, HEAD_DIM)
            chosen_values = value_blocks[picked_ids].reshape(CHOSEN * KEY_BLOCK, KV_HEADS, HEAD_DIM)
            all_keys = jnp.concatenate([chosen_keys, own_keys], axis=0).astype(jnp.float32)
            all_values = jnp.concatenate([chosen_values, own_values], axis=0).astype(jnp.float32)
            key_valid = jnp.broadcast_to(valid_row[:, None], (CHOSEN, KEY_BLOCK)).reshape(CHOSEN * KEY_BLOCK)
            far_mask = jnp.broadcast_to(key_valid[None, :], (QUERY_BLOCK, CHOSEN * KEY_BLOCK))
            full_mask = jnp.concatenate([far_mask, lower_mask], axis=1)
            scores = jnp.einsum('qngd,knd->ngqk', block_queries, all_keys) * HEAD_DIM ** (-0.5)
            scores = jnp.where(full_mask[None, None], scores, -jnp.inf)
            row_max = lax.optimization_barrier(jnp.max(scores, axis=-1, keepdims=True))
            weights = jnp.exp(scores - row_max)
            weights = (weights / lax.optimization_barrier(jnp.sum(weights, axis=-1, keepdims=True))).astype(jnp.bfloat16)
            mixed_out = jnp.einsum('ngqk,knd->qngd', weights.astype(jnp.float32), all_values)
            return mixed_out.reshape(QUERY_BLOCK, HEADS * HEAD_DIM).astype(jnp.bfloat16)
        mixed_rows = lax.map(one_block, jnp.arange(QBLOCKS, dtype=jnp.int32)).reshape(SEQ, HEADS * HEAD_DIM)
        share_cols = HEADS * HEAD_DIM // N_TP
        summed = jnp.zeros((SEQ, D), jnp.float32)
        for member in range(N_TP):
            partial_value = jnp.dot(mixed_rows[:, member * share_cols:(member + 1) * share_cols], out_weight[member * share_cols:(member + 1) * share_cols], preferred_element_type=jnp.float32).astype(jnp.bfloat16)
            summed = summed + lax.optimization_barrier(partial_value).astype(jnp.float32)
        mean_sq = lax.optimization_barrier(jnp.mean(summed * summed, axis=1, keepdims=True))
        return (summed * lax.rsqrt(mean_sq + norm_eps) * norm_gain.astype(jnp.float32)).astype(jnp.bfloat16)
    return lax.map(one_sequence, (tokens, chosen_owner, chosen_part))
```

```python
import functools

import jax
import jax.numpy as jnp
import numpy as np
from jax import lax
from jax.experimental import pallas as pl
from jax.experimental.pallas import tpu as pltpu
from jax.sharding import PartitionSpec as P

HEAD_DIM = 64
QUERY_BLOCK = 128
KEY_BLOCK = 64
LANES = 128
ROWS = 256
COLS = 256

rope_base = 10000.0
norm_eps = 1e-06
MESH = pl.DeviceIdType.MESH


def turn(u, cosine, sine):
    lane = lax.broadcasted_iota(jnp.int32, u.shape, 1)
    half = HEAD_DIM // 2
    swapped = jnp.where(
        lane % HEAD_DIM < half, pltpu.roll(u, LANES - half, 1), pltpu.roll(u, half, 1)
    )
    return u * cosine + swapped * sine


def spread(pair, head):
    wide = pair.astype(jnp.float32)
    swapped = pltpu.roll(wide, HEAD_DIM, 1)
    low = lax.broadcasted_iota(jnp.int32, wide.shape, 1) < HEAD_DIM
    in_low, in_high = (wide, swapped) if head == 0 else (swapped, wide)
    return jnp.concatenate(
        [jnp.where(low, in_low, 0.0), jnp.where(low, 0.0, in_high)], axis=0
    ).astype(jnp.bfloat16)


def kernel(
    devices, owner_hbm, part_hbm, tok_hbm, wq_hbm, wk_hbm, wv_hbm, ow_hbm, gain_hbm, trig_hbm, out,
    owner_ref, part_ref, gain, trig, small_sems, cosine, sine,
    tok, wq, wkv, ow, tok_sems, weight_sems,
    kv, send, pool, queries, mix, mix_other, ow_other, proj, ss, ss_other,
    kv_send, kv_recv, ow_sems, mix_send, mix_recv, ss_sems,
):
    me = lax.axis_index("kv")
    core = lax.axis_index("tp")
    other = 1 - core
    tokens = tok.shape[0]
    qblocks = tokens // QUERY_BLOCK
    chosen = owner_ref.shape[0]
    half = ow_other.shape[1]
    row_steps = tokens // ROWS
    per_q = QUERY_BLOCK // KEY_BLOCK

    key_width = wk_hbm.shape[1]

    def tok_copy(r):
        rows = pl.ds(pl.multiple_of(r * ROWS, ROWS), ROWS)
        return pltpu.make_async_copy(tok_hbm.at[rows], tok.at[rows], tok_sems.at[r])

    wk_copy = pltpu.make_async_copy(wk_hbm, wkv.at[:, pl.ds(0, key_width)], weight_sems.at[0])
    wv_copy = pltpu.make_async_copy(
        wv_hbm, wkv.at[:, pl.ds(key_width, key_width)], weight_sems.at[1]
    )
    wq_copy = pltpu.make_async_copy(wq_hbm, wq, weight_sems.at[2])
    ow_load = pltpu.make_async_copy(ow_hbm, ow, weight_sems.at[3])
    small = [
        pltpu.make_async_copy(trig_hbm, trig, small_sems.at[0]),
        pltpu.make_async_copy(owner_hbm, owner_ref, small_sems.at[1]),
        pltpu.make_async_copy(part_hbm, part_ref, small_sems.at[2]),
        pltpu.make_async_copy(gain_hbm, gain, small_sems.at[3]),
    ]
    small[0].start()
    wk_copy.start()
    wv_copy.start()
    for r in range(row_steps):
        tok_copy(r).start()
    for copy in small[1:]:
        copy.start()
    wq_copy.start()
    ow_load.start()

    barrier = pltpu.get_barrier_semaphore()

    @pl.loop(0, devices)
    def _(j):
        @pl.when(j != me)
        def _():
            pl.semaphore_signal(barrier, inc=1, device_id={"kv": j}, device_id_type=MESH)

    pl.semaphore_signal(barrier, inc=1, device_id={"tp": other}, device_id_type=MESH)

    small[0].wait()
    near_cos = trig[0:QUERY_BLOCK, :]
    near_sin = trig[QUERY_BLOCK : 2 * QUERY_BLOCK, :]

    @pl.loop(0, qblocks)
    def _(b):
        rows = pl.ds(pl.multiple_of(b * QUERY_BLOCK, QUERY_BLOCK), QUERY_BLOCK)
        at = 2 * QUERY_BLOCK + me * qblocks + b
        far_cos = trig[pl.ds(at, 1), :]
        far_sin = trig[pl.ds(at + devices * qblocks, 1), :]
        cosine[rows, :] = far_cos * near_cos - far_sin * near_sin
        sine[rows, :] = far_sin * near_cos + far_cos * near_sin

    wk_copy.wait()
    wv_copy.wait()

    @pl.loop(0, row_steps)
    def _(r):
        tok_copy(r).wait()
        rows = pl.ds(pl.multiple_of(r * ROWS, ROWS), ROWS)
        both = jnp.dot(
            tok[rows, :],
            wkv[...],
            preferred_element_type=jnp.float32,
        )
        keys = turn(both[:, :LANES], cosine[rows, :], sine[rows, :])
        joined = jnp.concatenate([keys, both[:, LANES:]], axis=1).astype(jnp.bfloat16)
        blocks = ROWS // KEY_BLOCK
        kv[pl.ds(r * blocks, blocks)] = joined.reshape(blocks, KEY_BLOCK, 2 * LANES)

    pl.semaphore_wait(barrier, devices)

    def place(src, row, s):
        return owner_ref[s, row] == src, part_ref[s, row]

    def wanted(dst, q):
        found = [place(me, dst * qblocks + q, s) for s in range(chosen)]
        return sum(jnp.where(here, at, 0) for here, at in found)

    def kv_copy(src, dst, to, q):
        return pltpu.make_async_remote_copy(
            src_ref=send.at[pl.ds(q * devices + dst, 1)],
            dst_ref=pool.at[pl.ds(q * devices + src, 1)],
            send_sem=kv_send.at[q, dst],
            recv_sem=kv_recv.at[q, src],
            device_id={"kv": to},
            device_id_type=MESH,
        )

    for copy in small[1:]:
        copy.wait()

    @pl.loop(0, qblocks)
    def _(q):
        @pl.loop(0, devices)
        def _(dst):
            @pl.when(dst > me)
            def _():
                send[pl.ds(q * devices + dst, 1)] = kv[pl.ds(wanted(dst, q), 1)]
                kv_copy(me, dst, dst, q).start()

            @pl.when(dst == me)
            def _():
                pool[pl.ds(q * devices + me, 1)] = kv[pl.ds(wanted(me, q), 1)]

            @pl.when(dst > me)
            def _():
                pool[pl.ds(q * devices + dst, 1)] = jnp.zeros(
                    (1, KEY_BLOCK, 2 * LANES), jnp.bfloat16
                )

    ow_copy = pltpu.make_async_remote_copy(
        src_ref=ow.at[:, pl.ds(pl.multiple_of(other * half, half), half)],
        dst_ref=ow_other,
        send_sem=ow_sems.at[0],
        recv_sem=ow_sems.at[1],
        device_id={"tp": other},
        device_id_type=MESH,
    )
    ow_load.wait()
    ow_copy.start()
    wq_copy.wait()

    @pl.loop(0, row_steps)
    def _(r):
        rows = pl.ds(pl.multiple_of(r * ROWS, ROWS), ROWS)
        for c in range(wq.shape[1] // COLS):
            part = jnp.dot(
                tok[rows, :], wq[:, c * COLS : (c + 1) * COLS], preferred_element_type=jnp.float32
            )
            for k in range(COLS // LANES):
                at = c * COLS + k * LANES
                queries[rows, at : at + LANES] = turn(
                    part[:, k * LANES : (k + 1) * LANES], cosine[rows, :], sine[rows, :]
                ).astype(jnp.bfloat16)

    kv_heads = key_width // HEAD_DIM
    slices = wq.shape[1] // LANES // kv_heads
    key_count = devices * KEY_BLOCK + QUERY_BLOCK

    def mix_copy(b):
        rows = pl.ds(pl.multiple_of(b * QUERY_BLOCK, QUERY_BLOCK), QUERY_BLOCK)
        return pltpu.make_async_remote_copy(
            src_ref=mix.at[rows],
            dst_ref=mix_other.at[rows],
            send_sem=mix_send.at[b],
            recv_sem=mix_recv.at[b],
            device_id={"tp": other},
            device_id_type=MESH,
        )

    def attend(b):
        row = me * qblocks + b

        @pl.loop(0, devices)
        def _(src):
            @pl.when(src < me)
            def _():
                kv_copy(src, src, src, b).wait_recv()

        rows = pl.ds(pl.multiple_of(b * QUERY_BLOCK, QUERY_BLOCK), QUERY_BLOCK)
        pieces = [pool[pl.ds(b * devices, devices)].reshape(devices * KEY_BLOCK, 2 * LANES)]
        lane = lax.broadcasted_iota(jnp.int32, (1, devices * KEY_BLOCK), 1) // KEY_BLOCK
        far = jnp.full((1, devices * KEY_BLOCK), -jnp.inf, jnp.float32)
        for src in range(devices):
            named = sum(jnp.where(place(src, row, s)[0], 1, 0) for s in range(chosen))
            far = jnp.where(lane == src, jnp.where(named > 0, 0.0, -jnp.inf), far)
        pieces.append(kv[pl.ds(b * per_q, per_q)].reshape(QUERY_BLOCK, 2 * LANES))
        near = jnp.where(
            lax.broadcasted_iota(jnp.int32, (slices * QUERY_BLOCK, QUERY_BLOCK), 0) % QUERY_BLOCK
            >= lax.broadcasted_iota(jnp.int32, (slices * QUERY_BLOCK, QUERY_BLOCK), 1),
            0.0,
            -jnp.inf,
        )
        bias = jnp.concatenate(
            [jnp.broadcast_to(far, (slices * QUERY_BLOCK, devices * KEY_BLOCK)), near], axis=1
        )
        both = jnp.concatenate(pieces, axis=0)
        for n in range(kv_heads):
            q = jnp.concatenate(
                [
                    queries[rows, (n * slices + m) * LANES : (n * slices + m + 1) * LANES]
                    for m in range(slices)
                ],
                axis=0,
            )
            scores = lax.dot_general(
                q,
                spread(both[:, :LANES], n),
                (((1,), (1,)), ((), ())),
                preferred_element_type=jnp.float32,
            )
            probs = []
            for side in range(2):
                s = scores[:, side * key_count : (side + 1) * key_count] * HEAD_DIM**-0.5 + bias
                e = jnp.exp(s - jnp.max(s, axis=1, keepdims=True))
                probs.append((e * (1.0 / jnp.sum(e, axis=1, keepdims=True))).astype(jnp.bfloat16))
            mixed = jnp.dot(
                jnp.concatenate(probs, axis=1),
                spread(both[:, LANES:], n),
                preferred_element_type=jnp.float32,
            ).astype(jnp.bfloat16)
            for m in range(slices):
                at = (n * slices + m) * LANES
                mix[rows, at : at + LANES] = mixed[m * QUERY_BLOCK : (m + 1) * QUERY_BLOCK]
        mix_copy(b).start()

    blocks_in = ROWS // QUERY_BLOCK

    def project(r):
        for k in range(blocks_in):
            mix_copy(r * blocks_in + k).wait_recv()
        rows = pl.ds(pl.multiple_of(r * ROWS, ROWS), ROWS)
        total = jnp.zeros((ROWS, LANES), jnp.float32)
        for c in range(half // COLS):
            mine = jnp.dot(
                mix[rows, :],
                ow[:, pl.ds(pl.multiple_of(core * half + c * COLS, COLS), COLS)],
                preferred_element_type=jnp.float32,
            ).astype(jnp.bfloat16)
            theirs = jnp.dot(
                mix_other[rows, :],
                ow_other[:, c * COLS : (c + 1) * COLS],
                preferred_element_type=jnp.float32,
            ).astype(jnp.bfloat16)
            added = mine.astype(jnp.float32) + theirs.astype(jnp.float32)
            proj[rows, c * COLS : (c + 1) * COLS] = added
            for k in range(COLS // LANES):
                piece = added[:, k * LANES : (k + 1) * LANES]
                total = total + piece * piece
        for k in range(ROWS // LANES):
            ss[r * (ROWS // LANES) + k] = jnp.sum(
                total[k * LANES : (k + 1) * LANES].T, axis=0, keepdims=True
            )

    ow_copy.wait_recv()

    @pl.loop(0, row_steps)
    def _(r):
        @pl.loop(0, blocks_in)
        def _(k):
            attend(r * blocks_in + k)

        @pl.when(r > 0)
        def _():
            project(r - 1)

    project(row_steps - 1)

    ss_copy = pltpu.make_async_remote_copy(
        src_ref=ss,
        dst_ref=ss_other,
        send_sem=ss_sems.at[0],
        recv_sem=ss_sems.at[1],
        device_id={"tp": other},
        device_id_type=MESH,
    )
    ss_copy.start()

    @pl.loop(0, qblocks)
    def _(q):
        @pl.loop(0, devices)
        def _(dst):
            @pl.when(dst > me)
            def _():
                kv_copy(me, dst, dst, q).wait_send()

    ow_copy.wait_send()

    @pl.loop(0, qblocks)
    def _(b):
        mix_copy(b).wait_send()

    ss_copy.wait()

    @pl.loop(0, qblocks)
    def _(b):
        rows = pl.ds(pl.multiple_of(b * LANES, LANES), LANES)
        scale = lax.rsqrt((ss[b] + ss_other[b]) / (2 * half) + norm_eps)
        scale = jnp.broadcast_to(scale, (LANES, LANES)).T
        for c in range(half // LANES):
            at = slice(c * LANES, (c + 1) * LANES)
            out[rows, at] = (proj[rows, at] * scale * gain[:, at]).astype(jnp.bfloat16)


def store_kernel(held, out, sems):
    def copy(b):
        rows = pl.ds(b * QUERY_BLOCK, QUERY_BLOCK)
        return pltpu.make_async_copy(held.at[rows], out.at[rows], sems.at[b])

    for b in range(sems.shape[0]):
        copy(b).start()
    for b in range(sems.shape[0]):
        copy(b).wait()


def trig_table(blocks):
    half_dim = HEAD_DIM // 2
    lane = np.arange(LANES)
    frequency = (rope_base ** (-(lane % half_dim) / half_dim)).astype(np.float32)
    sign = np.where(lane % HEAD_DIM < half_dim, -1.0, 1.0)
    near = np.arange(QUERY_BLOCK)[:, None] * frequency.astype(np.float64)
    far = (np.arange(blocks)[:, None] * np.float32(QUERY_BLOCK) * frequency).astype(np.float64)
    parts = [np.cos(near), sign * np.sin(near), np.cos(far), sign * np.sin(far)]
    return np.concatenate(parts, axis=0).astype(np.float32)


def body(
    tokens, query_weight, key_weight, value_weight, out_weight, norm_gain, chosen_owner, chosen_part
):
    row_data = tokens[0]
    count = row_data.shape[0]
    devices = lax.axis_size("kv")
    qblocks = count // QUERY_BLOCK
    heads_width = query_weight.shape[1]
    half = norm_gain.shape[0]
    hbm = pl.BlockSpec(memory_space=pl.ANY)
    vmem = pl.BlockSpec(memory_space=pltpu.VMEM)
    bf16, f32 = jnp.bfloat16, jnp.float32
    slots = chosen_owner.shape[1:][::-1]
    trig = trig_table(devices * qblocks)
    operands = [
        chosen_owner[0].T, chosen_part[0].T, row_data, query_weight, key_weight, value_weight,
        out_weight, norm_gain[None], jnp.asarray(trig),
    ]
    operands = [pltpu.with_memory_space_constraint(x, pltpu.HBM) for x in operands]
    result = pl.pallas_call(
        functools.partial(kernel, devices),
        out_shape=pltpu.VMEM((count, half), bf16),
        in_specs=[hbm] * len(operands),
        out_specs=vmem,
        scratch_shapes=[
            pltpu.SMEM(slots, jnp.int32),
            pltpu.SMEM(slots, jnp.int32),
            pltpu.VMEM((1, half), f32),
            pltpu.VMEM(trig.shape, f32),
            pltpu.SemaphoreType.DMA((4,)),
            pltpu.VMEM((count, LANES), f32),
            pltpu.VMEM((count, LANES), f32),
            pltpu.VMEM(row_data.shape, bf16),
            pltpu.VMEM(query_weight.shape, bf16),
            pltpu.VMEM((key_weight.shape[0], 2 * key_weight.shape[1]), bf16),
            pltpu.VMEM(out_weight.shape, bf16),
            pltpu.SemaphoreType.DMA((count // ROWS,)),
            pltpu.SemaphoreType.DMA((4,)),
            pltpu.VMEM((count // KEY_BLOCK, KEY_BLOCK, 2 * LANES), bf16),
            pltpu.VMEM((devices * qblocks, KEY_BLOCK, 2 * LANES), bf16),
            pltpu.VMEM((devices * qblocks, KEY_BLOCK, 2 * LANES), bf16),
            pltpu.VMEM((count, heads_width), bf16),
            pltpu.VMEM((count, heads_width), bf16),
            pltpu.VMEM((count, heads_width), bf16),
            pltpu.VMEM((out_weight.shape[0], half), bf16),
            pltpu.VMEM((count, half), f32),
            pltpu.VMEM((qblocks, 1, LANES), f32),
            pltpu.VMEM((qblocks, 1, LANES), f32),
            pltpu.SemaphoreType.DMA((qblocks, devices)),
            pltpu.SemaphoreType.DMA((qblocks, devices)),
            pltpu.SemaphoreType.DMA((2,)),
            pltpu.SemaphoreType.DMA((qblocks,)),
            pltpu.SemaphoreType.DMA((qblocks,)),
            pltpu.SemaphoreType.DMA((2,)),
        ],
        compiler_params=pltpu.CompilerParams(
            collective_id=0, has_side_effects=True, vmem_limit_bytes=48 * 1024 * 1024
        ),
    )(*operands)
    return pl.pallas_call(
        store_kernel,
        out_shape=jax.ShapeDtypeStruct((count, half), bf16),
        in_specs=[vmem],
        out_specs=hbm,
        scratch_shapes=[pltpu.SemaphoreType.DMA((qblocks,))],
        compiler_params=pltpu.CompilerParams(vmem_limit_bytes=4 * 1024 * 1024),
    )(pltpu.with_memory_space_constraint(result, pltpu.VMEM))[None]


def solution(mesh):
    placed = (
        P("dp", "kv", None),
        P(None, "tp"),
        P(None, "tp"),
        P(None, "tp"),
        P("tp", None),
        P("tp"),
        P("dp", None, None),
        P("dp", None, None),
    )
    return jax.shard_map(
        body, mesh=mesh, in_specs=placed, out_specs=P("dp", "kv", "tp"), check_vma=False
    )
```

```python
import functools

import jax
import jax.numpy as jnp
import numpy as np
from jax import lax
from jax.experimental import pallas as pl
from jax.experimental.pallas import tpu as pltpu
from jax.sharding import PartitionSpec as P

HEAD_DIM = 64
QUERY_BLOCK = 128
KEY_BLOCK = 64
LANES = 128
ROWS = 256
COLS = 256

rope_base = 10000.0
norm_eps = 1e-06
hidden = -1e38
MESH = pl.DeviceIdType.MESH


def low_lanes(shape):
    return lax.broadcasted_iota(jnp.int32, shape, 1) < HEAD_DIM


def turn(u, cosine, sine):
    lane = lax.broadcasted_iota(jnp.int32, u.shape, 1)
    half = HEAD_DIM // 2
    swapped = jnp.where(
        lane % HEAD_DIM < half, pltpu.roll(u, LANES - half, 1), pltpu.roll(u, half, 1)
    )
    return u * cosine + swapped * sine


def kernel(
    devices, owner_hbm, part_hbm, tok_hbm, wq_hbm, wk_hbm, wv_hbm, ow_hbm, gain_hbm, trig_hbm, out,
    owner_ref, part_ref, gain, trig, small_sems, cosine, sine, eye, causal,
    tok, wq, wkv, ow, tok_sems, weight_sems, ow_load_sems,
    kv, send, pool, queries, mix, mix_other, ow_other, partial, proj,
    kv_send, kv_recv, ow_sems, mix_send, mix_recv,
):
    me = lax.axis_index("kv")
    core = lax.axis_index("tp")
    other = 1 - core
    tokens = tok.shape[0]
    qblocks = tokens // QUERY_BLOCK
    chosen = owner_ref.shape[0]
    half = gain.shape[1]
    row_steps = tokens // ROWS
    per_q = QUERY_BLOCK // KEY_BLOCK
    key_width = wk_hbm.shape[1]
    slices = wq.shape[1] // LANES
    heads = wq.shape[1] // HEAD_DIM
    bf16, f32 = jnp.bfloat16, jnp.float32

    def tok_copy(r):
        rows = pl.ds(pl.multiple_of(r * ROWS, ROWS), ROWS)
        return pltpu.make_async_copy(tok_hbm.at[rows], tok.at[rows], tok_sems.at[r])

    wk_copy = pltpu.make_async_copy(wk_hbm, wkv.at[:, pl.ds(0, key_width)], weight_sems.at[0])
    wv_copy = pltpu.make_async_copy(
        wv_hbm, wkv.at[:, pl.ds(key_width, key_width)], weight_sems.at[1]
    )
    wq_copy = pltpu.make_async_copy(wq_hbm, wq, weight_sems.at[2])
    ow_loads = []
    for m in range(slices):
        for g in range(2):
            ow_loads.append(
                pltpu.make_async_copy(
                    ow_hbm.at[pl.ds((g * slices + m) * HEAD_DIM, HEAD_DIM)],
                    ow.at[pl.ds((2 * m + g) * HEAD_DIM, HEAD_DIM)],
                    ow_load_sems.at[2 * m + g],
                )
            )
    small = [
        pltpu.make_async_copy(trig_hbm, trig, small_sems.at[0]),
        pltpu.make_async_copy(owner_hbm, owner_ref, small_sems.at[1]),
        pltpu.make_async_copy(part_hbm, part_ref, small_sems.at[2]),
        pltpu.make_async_copy(gain_hbm, gain, small_sems.at[3]),
    ]
    small[0].start()
    wk_copy.start()
    wv_copy.start()
    for r in range(row_steps):
        tok_copy(r).start()
    for copy in small[1:]:
        copy.start()

    barrier = pltpu.get_barrier_semaphore()

    @pl.loop(0, devices)
    def _(j):
        @pl.when(j != me)
        def _():
            pl.semaphore_signal(barrier, inc=1, device_id={"kv": j}, device_id_type=MESH)

    pl.semaphore_signal(barrier, inc=1, device_id={"tp": other}, device_id_type=MESH)

    square = (QUERY_BLOCK, QUERY_BLOCK)
    first = lax.broadcasted_iota(jnp.int32, square, 0)
    second = lax.broadcasted_iota(jnp.int32, square, 1)
    eye[...] = jnp.where(first == second, 1.0, 0.0).astype(bf16)
    causal[...] = jnp.where(second >= first, 0.0, hidden).astype(bf16)

    small[0].wait()
    near_cos = trig[0:QUERY_BLOCK, :]
    near_sin = trig[QUERY_BLOCK : 2 * QUERY_BLOCK, :]

    @pl.loop(0, qblocks)
    def _(b):
        rows = pl.ds(pl.multiple_of(b * QUERY_BLOCK, QUERY_BLOCK), QUERY_BLOCK)
        at = 2 * QUERY_BLOCK + me * qblocks + b
        far_cos = trig[pl.ds(at, 1), :]
        far_sin = trig[pl.ds(at + devices * qblocks, 1), :]
        cosine[rows, :] = far_cos * near_cos - far_sin * near_sin
        sine[rows, :] = far_sin * near_cos + far_cos * near_sin

    wk_copy.wait()
    wv_copy.wait()

    @pl.loop(0, row_steps)
    def _(r):
        tok_copy(r).wait()

        @pl.when(r == 0)
        def _():
            wq_copy.start()
            for copy in ow_loads:
                copy.start()

        rows = pl.ds(pl.multiple_of(r * ROWS, ROWS), ROWS)
        both = jnp.dot(tok[rows, :], wkv[...], preferred_element_type=f32)
        keys = turn(both[:, :LANES], cosine[rows, :], sine[rows, :])
        joined = jnp.concatenate([keys, both[:, LANES:]], axis=1).astype(bf16)
        blocks = ROWS // KEY_BLOCK
        kv[pl.ds(r * blocks, blocks)] = joined.reshape(blocks, KEY_BLOCK, 2 * LANES)

    for copy in small[1:]:
        copy.wait()
    pl.semaphore_wait(barrier, devices)

    def place(src, row, s):
        return owner_ref[s, row] == src, part_ref[s, row]

    def wanted(dst, q):
        found = [place(me, dst * qblocks + q, s) for s in range(chosen)]
        return sum(jnp.where(here, at, 0) for here, at in found)

    def kv_copy(src, dst, to, q):
        return pltpu.make_async_remote_copy(
            src_ref=send.at[pl.ds(q * devices + dst, 1)],
            dst_ref=pool.at[pl.ds(q * devices + src, 1)],
            send_sem=kv_send.at[q, dst],
            recv_sem=kv_recv.at[q, src],
            device_id={"kv": to},
            device_id_type=MESH,
        )

    @pl.loop(0, qblocks)
    def _(q):
        @pl.loop(0, devices - 1)
        def _(step):
            dst = devices - 1 - step

            @pl.when(dst > me)
            def _():
                send[pl.ds(q * devices + dst, 1)] = kv[pl.ds(wanted(dst, q), 1)]
                kv_copy(me, dst, dst, q).start()

    @pl.loop(0, qblocks)
    def _(q):
        pool[pl.ds(q * devices + me, 1)] = kv[pl.ds(wanted(me, q), 1)]

        @pl.loop(0, devices)
        def _(src):
            @pl.when(src > me)
            def _():
                pool[pl.ds(q * devices + src, 1)] = jnp.zeros((1, KEY_BLOCK, 2 * LANES), bf16)

    ow_copy = pltpu.make_async_remote_copy(
        src_ref=ow,
        dst_ref=ow_other,
        send_sem=ow_sems.at[0],
        recv_sem=ow_sems.at[1],
        device_id={"tp": other},
        device_id_type=MESH,
    )
    wq_copy.wait()

    @pl.loop(0, row_steps)
    def _(r):
        @pl.when(r == 1)
        def _():
            for copy in ow_loads:
                copy.wait()
            ow_copy.start()

        rows = pl.ds(pl.multiple_of(r * ROWS, ROWS), ROWS)
        scale = HEAD_DIM**-0.5
        scaled_cos, scaled_sin = cosine[rows, :] * scale, sine[rows, :] * scale
        for c in range(wq.shape[1] // COLS):
            part = jnp.dot(
                tok[rows, :], wq[:, c * COLS : (c + 1) * COLS], preferred_element_type=f32
            )
            for k in range(COLS // LANES):
                turned = turn(part[:, k * LANES : (k + 1) * LANES], scaled_cos, scaled_sin)
                away = pltpu.roll(turned, HEAD_DIM, 1)
                for j in range(2):
                    head = 2 * (c * (COLS // LANES) + k) + j
                    group, m = head // slices, head % slices
                    lanes = slice(group * HEAD_DIM, (group + 1) * HEAD_DIM)
                    at = m * LANES + group * HEAD_DIM
                    queries[rows, at : at + HEAD_DIM] = (
                        turned if group == j else away
                    )[:, lanes].astype(bf16)

    key_count = devices * KEY_BLOCK + QUERY_BLOCK

    def mix_copy(b):
        rows = pl.ds(pl.multiple_of(b * QUERY_BLOCK, QUERY_BLOCK), QUERY_BLOCK)
        return pltpu.make_async_remote_copy(
            src_ref=mix.at[rows],
            dst_ref=mix_other.at[rows],
            send_sem=mix_send.at[b],
            recv_sem=mix_recv.at[b],
            device_id={"tp": other},
            device_id_type=MESH,
        )

    low_mask = jnp.where(low_lanes((key_count, LANES)), 1.0, 0.0).astype(bf16)
    high_mask = jnp.where(low_lanes((key_count, LANES)), 0.0, 1.0).astype(bf16)

    def attend(b):
        row = me * qblocks + b

        @pl.loop(0, devices)
        def _(src):
            @pl.when(src < me)
            def _():
                kv_copy(src, src, src, b).wait_recv()

        rows = pl.ds(pl.multiple_of(b * QUERY_BLOCK, QUERY_BLOCK), QUERY_BLOCK)
        far = pool[pl.ds(b * devices, devices)].reshape(devices * KEY_BLOCK, 2 * LANES)
        near = kv[pl.ds(b * per_q, per_q)].reshape(QUERY_BLOCK, 2 * LANES)
        both = jnp.concatenate([far, near], axis=0)
        keys, values = both[:, :LANES], both[:, LANES:]
        bias = []
        for src in range(devices):
            named = sum(jnp.where(place(src, row, s)[0], 1, 0) for s in range(chosen))
            bias.append(
                jnp.full((KEY_BLOCK, LANES), jnp.where(named > 0, 0.0, hidden), f32).astype(bf16)
            )
        bias = jnp.concatenate(bias + [causal[...]], axis=0)
        wide_keys = jnp.concatenate(
            [
                jnp.concatenate([keys * low_mask, bias], axis=1),
                jnp.concatenate([keys * high_mask, bias], axis=1),
            ],
            axis=0,
        )
        wide_values = jnp.concatenate(
            [
                jnp.concatenate([values * low_mask, low_mask], axis=1),
                jnp.concatenate([values * high_mask, high_mask], axis=1),
            ],
            axis=0,
        )
        for pair in range(0, slices, 2):
            q = jnp.concatenate(
                [
                    jnp.concatenate([queries[rows, m * LANES : (m + 1) * LANES], eye[...]], axis=1)
                    for m in (pair, pair + 1)
                ],
                axis=0,
            )
            scores = lax.dot_general(
                q, wide_keys, (((1,), (1,)), ((), ())), preferred_element_type=f32
            )
            weights = []
            for side in range(2):
                s = scores[:, side * key_count : (side + 1) * key_count]
                weights.append(jnp.exp(s - jnp.max(s, axis=1, keepdims=True)).astype(bf16))
            mixed = jnp.dot(
                jnp.concatenate(weights, axis=1), wide_values, preferred_element_type=f32
            )
            mixed = (mixed[:, :LANES] / mixed[:, LANES:]).astype(bf16)
            for k in range(2):
                at = (pair + k) * LANES
                mix[rows, at : at + LANES] = mixed[k * QUERY_BLOCK : (k + 1) * QUERY_BLOCK]
        mix_copy(b).start()

    def part_of(left, right, rows, side, c):
        cols = pl.ds(pl.multiple_of(side * half + c * COLS, COLS), COLS)
        return jnp.dot(left[rows, :], right[:, cols], preferred_element_type=f32).astype(bf16)

    def project_mine(start, count):
        rows = pl.ds(start, count)
        for n, side in enumerate((other, core)):
            for c in range(half // COLS):
                at = n * half + c * COLS
                partial[:count, at : at + COLS] = part_of(mix, ow, rows, side, c)

    def project(start, count, ready=False):
        rows = pl.ds(start, count)
        total = jnp.zeros((count, LANES), f32)
        for n, side in enumerate((other, core)):
            for c in range(half // COLS):
                at = n * half + c * COLS
                mine = partial[:count, at : at + COLS] if ready else part_of(mix, ow, rows, side, c)
                theirs = part_of(mix_other, ow_other, rows, side, c)
                added = mine.astype(f32) + theirs.astype(f32)
                if side is core:
                    proj[:count, c * COLS : (c + 1) * COLS] = added
                for k in range(COLS // LANES):
                    piece = added[:, k * LANES : (k + 1) * LANES]
                    total = total + piece * piece
        scale = lax.rsqrt(jnp.sum(total, axis=1, keepdims=True) / (2 * half) + norm_eps)
        for c in range(half // LANES):
            at = slice(c * LANES, (c + 1) * LANES)
            out[rows, at] = (proj[:count, at] * scale * gain[:, at]).astype(bf16)

    blocks_in = ROWS // QUERY_BLOCK

    @pl.loop(0, row_steps)
    def _(r):
        @pl.loop(0, blocks_in)
        def _(k):
            attend(r * blocks_in + k)

            @pl.when(jnp.logical_and(r == 1, k == 0))
            def _():
                ow_copy.wait_recv()

            @pl.when(jnp.logical_and(r > 0, k == 0))
            def _():
                for j in range(blocks_in):
                    mix_copy((r - 1) * blocks_in + j).wait_recv()
                project(pl.multiple_of((r - 1) * ROWS, ROWS), ROWS)

    for b in range(qblocks - blocks_in, qblocks - 1):
        mix_copy(b).wait_recv()
        project(b * QUERY_BLOCK, QUERY_BLOCK)
    last = qblocks - 1
    project_mine(last * QUERY_BLOCK, QUERY_BLOCK)

    @pl.loop(0, qblocks)
    def _(q):
        @pl.loop(0, devices)
        def _(dst):
            @pl.when(dst > me)
            def _():
                kv_copy(me, dst, dst, q).wait_send()

    ow_copy.wait_send()

    @pl.loop(0, last)
    def _(b):
        mix_copy(b).wait_send()

    mix_copy(last).wait_recv()
    project(last * QUERY_BLOCK, QUERY_BLOCK, ready=True)
    mix_copy(last).wait_send()


def store_kernel(held, out, sems):
    def copy(b):
        rows = pl.ds(b * QUERY_BLOCK, QUERY_BLOCK)
        return pltpu.make_async_copy(held.at[rows], out.at[rows], sems.at[b])

    for b in range(sems.shape[0]):
        copy(b).start()
    for b in range(sems.shape[0]):
        copy(b).wait()


def trig_table(blocks):
    half_dim = HEAD_DIM // 2
    lane = np.arange(LANES)
    frequency = (rope_base ** (-(lane % half_dim) / half_dim)).astype(np.float32)
    sign = np.where(lane % HEAD_DIM < half_dim, -1.0, 1.0)
    near = np.arange(QUERY_BLOCK)[:, None] * frequency.astype(np.float64)
    far = (np.arange(blocks)[:, None] * np.float32(QUERY_BLOCK) * frequency).astype(np.float64)
    parts = [np.cos(near), sign * np.sin(near), np.cos(far), sign * np.sin(far)]
    return np.concatenate(parts, axis=0).astype(np.float32)


def body(
    tokens, query_weight, key_weight, value_weight, out_weight, norm_gain, chosen_owner, chosen_part
):
    row_data = tokens[0]
    count = row_data.shape[0]
    devices = lax.axis_size("kv")
    qblocks = count // QUERY_BLOCK
    heads_width = query_weight.shape[1]
    half = norm_gain.shape[0]
    hbm = pl.BlockSpec(memory_space=pl.ANY)
    vmem = pl.BlockSpec(memory_space=pltpu.VMEM)
    bf16, f32 = jnp.bfloat16, jnp.float32
    slots = chosen_owner.shape[1:][::-1]
    trig = trig_table(devices * qblocks)
    operands = [
        chosen_owner[0].T, chosen_part[0].T, row_data, query_weight, key_weight, value_weight,
        out_weight, norm_gain[None], jnp.asarray(trig),
    ]
    operands = [pltpu.with_memory_space_constraint(x, pltpu.HBM) for x in operands]
    result = pl.pallas_call(
        functools.partial(kernel, devices),
        out_shape=pltpu.VMEM((count, half), bf16),
        in_specs=[hbm] * len(operands),
        out_specs=vmem,
        scratch_shapes=[
            pltpu.SMEM(slots, jnp.int32),
            pltpu.SMEM(slots, jnp.int32),
            pltpu.VMEM((1, half), f32),
            pltpu.VMEM(trig.shape, f32),
            pltpu.SemaphoreType.DMA((4,)),
            pltpu.VMEM((count, LANES), f32),
            pltpu.VMEM((count, LANES), f32),
            pltpu.VMEM((QUERY_BLOCK, QUERY_BLOCK), bf16),
            pltpu.VMEM((QUERY_BLOCK, QUERY_BLOCK), bf16),
            pltpu.VMEM(row_data.shape, bf16),
            pltpu.VMEM(query_weight.shape, bf16),
            pltpu.VMEM((key_weight.shape[0], 2 * key_weight.shape[1]), bf16),
            pltpu.VMEM(out_weight.shape, bf16),
            pltpu.SemaphoreType.DMA((count // ROWS,)),
            pltpu.SemaphoreType.DMA((3,)),
            pltpu.SemaphoreType.DMA((heads_width // HEAD_DIM,)),
            pltpu.VMEM((count // KEY_BLOCK, KEY_BLOCK, 2 * LANES), bf16),
            pltpu.VMEM((devices * qblocks, KEY_BLOCK, 2 * LANES), bf16),
            pltpu.VMEM((devices * qblocks, KEY_BLOCK, 2 * LANES), bf16),
            pltpu.VMEM((count, heads_width), bf16),
            pltpu.VMEM((count, heads_width), bf16),
            pltpu.VMEM((count, heads_width), bf16),
            pltpu.VMEM(out_weight.shape, bf16),
            pltpu.VMEM((QUERY_BLOCK, 2 * half), bf16),
            pltpu.VMEM((ROWS, half), f32),
            pltpu.SemaphoreType.DMA((qblocks, devices)),
            pltpu.SemaphoreType.DMA((qblocks, devices)),
            pltpu.SemaphoreType.DMA((2,)),
            pltpu.SemaphoreType.DMA((qblocks,)),
            pltpu.SemaphoreType.DMA((qblocks,)),
        ],
        compiler_params=pltpu.CompilerParams(
            collective_id=0, has_side_effects=True, vmem_limit_bytes=48 * 1024 * 1024
        ),
    )(*operands)
    return pl.pallas_call(
        store_kernel,
        out_shape=jax.ShapeDtypeStruct((count, half), bf16),
        in_specs=[vmem],
        out_specs=hbm,
        scratch_shapes=[pltpu.SemaphoreType.DMA((qblocks,))],
        compiler_params=pltpu.CompilerParams(vmem_limit_bytes=4 * 1024 * 1024),
    )(pltpu.with_memory_space_constraint(result, pltpu.VMEM))[None]


def solution(mesh):
    placed = (
        P("dp", "kv", None),
        P(None, "tp"),
        P(None, "tp"),
        P(None, "tp"),
        P("tp", None),
        P("tp"),
        P("dp", None, None),
        P("dp", None, None),
    )
    return jax.shard_map(
        body, mesh=mesh, in_specs=placed, out_specs=P("dp", "kv", "tp"), check_vma=False
    )
```

```python
import functools

import jax
import jax.numpy as jnp
import numpy as np
from jax import lax
from jax.experimental import pallas as pl
from jax.experimental.pallas import tpu as pltpu
from jax.sharding import PartitionSpec as P

HEAD_DIM = 64
QUERY_BLOCK = 128
KEY_BLOCK = 64
LANES = 128
ROWS = 256
COLS = 256

rope_base = 10000.0
norm_eps = 1e-06
hidden = -1e38
MESH = pl.DeviceIdType.MESH


def low_lanes(shape):
    return lax.broadcasted_iota(jnp.int32, shape, 1) < HEAD_DIM


def turn(u, cosine, sine):
    lane = lax.broadcasted_iota(jnp.int32, u.shape, 1)
    half = HEAD_DIM // 2
    swapped = jnp.where(
        lane % HEAD_DIM < half, pltpu.roll(u, LANES - half, 1), pltpu.roll(u, half, 1)
    )
    return u * cosine + swapped * sine


def kernel(
    devices, owner_hbm, part_hbm, tok_hbm, wq_hbm, wk_hbm, wv_hbm, ow_hbm, gain_hbm, trig_hbm, out,
    owner_ref, part_ref, gain, trig, small_sems, cosine, sine, eye, causal,
    tok, wq, wkv, ow, tok_sems, weight_sems,
    kv, send, pool, queries, keys_now, values_now, scores, weights, mix, mix_other, ow_other, partial, proj, ss, ss_other,
    kv_send, kv_recv, ow_sems, mix_send, mix_recv, ss_send, ss_recv,
):
    me = lax.axis_index("kv")
    core = lax.axis_index("tp")
    other = 1 - core
    tokens = tok.shape[0]
    qblocks = tokens // QUERY_BLOCK
    chosen = owner_ref.shape[0]
    half = gain.shape[1]
    row_steps = tokens // ROWS
    per_q = QUERY_BLOCK // KEY_BLOCK
    key_width = wk_hbm.shape[1]
    slices = wq.shape[1] // LANES
    heads = wq.shape[1] // HEAD_DIM
    bf16, f32 = jnp.bfloat16, jnp.float32

    part_rows = tokens // 2

    def tok_copy(r):
        rows = pl.ds(pl.multiple_of(r * part_rows, part_rows), part_rows)
        return pltpu.make_async_copy(tok_hbm.at[rows], tok.at[rows], tok_sems.at[r])

    wk_copy = pltpu.make_async_copy(wk_hbm, wkv.at[:, pl.ds(0, key_width)], weight_sems.at[0])
    wv_copy = pltpu.make_async_copy(
        wv_hbm, wkv.at[:, pl.ds(key_width, key_width)], weight_sems.at[0]
    )
    wq_copy = pltpu.make_async_copy(wq_hbm, wq, weight_sems.at[1])
    ow_loads = []
    for m in range(slices):
        for g in range(2):
            ow_loads.append(
                pltpu.make_async_copy(
                    ow_hbm.at[pl.ds((g * slices + m) * HEAD_DIM, HEAD_DIM)],
                    ow.at[pl.ds((2 * m + g) * HEAD_DIM, HEAD_DIM)],
                    weight_sems.at[2],
                )
            )
    small = [
        pltpu.make_async_copy(trig_hbm, trig, small_sems.at[0]),
        pltpu.make_async_copy(owner_hbm, owner_ref, small_sems.at[1]),
        pltpu.make_async_copy(part_hbm, part_ref, small_sems.at[2]),
        pltpu.make_async_copy(gain_hbm, gain, small_sems.at[3]),
    ]
    small[0].start()
    wk_copy.start()
    wv_copy.start()
    tok_copy(0).start()
    tok_copy(1).start(priority=1)
    for copy in small[1:]:
        copy.start(priority=1)

    barrier = pltpu.get_barrier_semaphore()

    @pl.loop(0, devices)
    def _(j):
        @pl.when(j != me)
        def _():
            pl.semaphore_signal(barrier, inc=1, device_id={"kv": j}, device_id_type=MESH)

    pl.semaphore_signal(barrier, inc=1, device_id={"tp": other}, device_id_type=MESH)

    square = (QUERY_BLOCK, QUERY_BLOCK)
    first = lax.broadcasted_iota(jnp.int32, square, 0)
    second = lax.broadcasted_iota(jnp.int32, square, 1)
    eye[...] = jnp.where(first == second, 1.0, 0.0).astype(bf16)
    causal[...] = jnp.where(first >= second, 0.0, hidden).astype(bf16)

    small[0].wait()
    near_cos = trig[0:QUERY_BLOCK, :]
    near_sin = trig[QUERY_BLOCK : 2 * QUERY_BLOCK, :]

    @pl.loop(0, qblocks)
    def _(b):
        rows = pl.ds(pl.multiple_of(b * QUERY_BLOCK, QUERY_BLOCK), QUERY_BLOCK)
        at = 2 * QUERY_BLOCK + me * qblocks + b
        far_cos = trig[pl.ds(at, 1), :]
        far_sin = trig[pl.ds(at + devices * qblocks, 1), :]
        cosine[rows, :] = far_cos * near_cos - far_sin * near_sin
        sine[rows, :] = far_sin * near_cos + far_cos * near_sin

    pltpu.make_async_copy(wkv, wkv, weight_sems.at[0]).wait()

    @pl.loop(0, 2)
    def _(r):
        tok_copy(r).wait()

        @pl.when(r == 0)
        def _():
            wq_copy.start(priority=1)
            for copy in ow_loads:
                copy.start(priority=1)

        rows = pl.ds(pl.multiple_of(r * part_rows, part_rows), part_rows)
        both = jnp.dot(tok[rows, :], wkv[...], preferred_element_type=f32)
        keys = turn(both[:, :LANES], cosine[rows, :], sine[rows, :])
        joined = jnp.concatenate([keys, both[:, LANES:]], axis=1).astype(bf16)
        blocks = part_rows // KEY_BLOCK
        kv[pl.ds(r * blocks, blocks)] = joined.reshape(blocks, KEY_BLOCK, 2 * LANES)

    for copy in small[1:]:
        copy.wait()
    pl.semaphore_wait(barrier, devices)

    def place(src, row, s):
        return owner_ref[s, row] == src, part_ref[s, row]

    def wanted(dst, q):
        found = [place(me, dst * qblocks + q, s) for s in range(chosen)]
        return sum(jnp.where(here, at, 0) for here, at in found)

    def kv_copy(src, dst, to, q):
        return pltpu.make_async_remote_copy(
            src_ref=send.at[pl.ds(dst * qblocks + q, 1)],
            dst_ref=pool.at[pl.ds(q * devices + src, 1)],
            send_sem=kv_send.at[dst],
            recv_sem=kv_recv.at[q],
            device_id={"kv": to},
            device_id_type=MESH,
        )

    @pl.loop(0, qblocks)
    def _(q):
        @pl.loop(0, devices - 1)
        def _(step):
            dst = devices - 1 - step

            @pl.when(dst > me)
            def _():
                send[pl.ds(dst * qblocks + q, 1)] = kv[pl.ds(wanted(dst, q), 1)]
                kv_copy(me, dst, dst, q).start()

    @pl.loop(0, qblocks)
    def _(q):
        pool[pl.ds(q * devices + me, 1)] = kv[pl.ds(wanted(me, q), 1)]

        @pl.loop(0, devices)
        def _(src):
            @pl.when(src > me)
            def _():
                pool[pl.ds(q * devices + src, 1)] = jnp.zeros((1, KEY_BLOCK, 2 * LANES), bf16)

    ow_copy = pltpu.make_async_remote_copy(
        src_ref=ow,
        dst_ref=ow_other,
        send_sem=ow_sems.at[0],
        recv_sem=ow_sems.at[1],
        device_id={"tp": other},
        device_id_type=MESH,
    )
    wq_copy.wait()

    @pl.loop(0, row_steps)
    def _(r):
        @pl.when(r == 1)
        def _():
            pltpu.make_async_copy(ow, ow, weight_sems.at[2]).wait()
            ow_copy.start()

        rows = pl.ds(pl.multiple_of(r * ROWS, ROWS), ROWS)
        scale = HEAD_DIM**-0.5
        scaled_cos, scaled_sin = cosine[rows, :] * scale, sine[rows, :] * scale
        for c in range(wq.shape[1] // COLS):
            part = jnp.dot(
                tok[rows, :], wq[:, c * COLS : (c + 1) * COLS], preferred_element_type=f32
            )
            for k in range(COLS // LANES):
                turned = turn(part[:, k * LANES : (k + 1) * LANES], scaled_cos, scaled_sin)
                away = pltpu.roll(turned, HEAD_DIM, 1)
                for j in range(2):
                    head = 2 * (c * (COLS // LANES) + k) + j
                    group, m = head // slices, head % slices
                    lanes = slice(group * HEAD_DIM, (group + 1) * HEAD_DIM)
                    at = m * LANES + group * HEAD_DIM
                    queries[rows, at : at + HEAD_DIM] = (
                        turned if group == j else away
                    )[:, lanes].astype(bf16)

    key_count = devices * KEY_BLOCK + QUERY_BLOCK

    blocks_in = ROWS // QUERY_BLOCK
    last = qblocks - 1

    def group_of(b):
        return b // blocks_in + jnp.where(b == last, 1, 0)

    def wait_mix(first, count):
        rows = pl.ds(pl.multiple_of(first * QUERY_BLOCK, QUERY_BLOCK), count * QUERY_BLOCK)
        landed = mix_other.at[rows]
        pltpu.make_async_copy(landed, landed, mix_recv.at[group_of(first)]).wait()

    def mix_copy(b):
        rows = pl.ds(pl.multiple_of(b * QUERY_BLOCK, QUERY_BLOCK), QUERY_BLOCK)
        return pltpu.make_async_remote_copy(
            src_ref=mix.at[rows],
            dst_ref=mix_other.at[rows],
            send_sem=mix_send.at[0],
            recv_sem=mix_recv.at[group_of(b)],
            device_id={"tp": other},
            device_id_type=MESH,
        )

    low_mask = jnp.where(low_lanes((key_count, LANES)), 1.0, 0.0).astype(bf16)
    high_mask = jnp.where(low_lanes((key_count, LANES)), 0.0, 1.0).astype(bf16)

    def attend(b):
        row = me * qblocks + b

        for n in range(1, devices):

            @pl.when(me == n)
            def _():
                landed = pool.at[pl.ds(b * devices, n)]
                pltpu.make_async_copy(landed, landed, kv_recv.at[b]).wait()

        rows = pl.ds(pl.multiple_of(b * QUERY_BLOCK, QUERY_BLOCK), QUERY_BLOCK)
        far = pool[pl.ds(b * devices, devices)].reshape(devices * KEY_BLOCK, 2 * LANES)
        near = kv[pl.ds(b * per_q, per_q)].reshape(QUERY_BLOCK, 2 * LANES)
        both = jnp.concatenate([far, near], axis=0)
        keys, values = both[:, :LANES], both[:, LANES:]
        owner = lax.broadcasted_iota(jnp.int32, (1, devices * KEY_BLOCK), 1) // KEY_BLOCK
        bias = jnp.full((1, devices * KEY_BLOCK), hidden, f32)
        for s in range(chosen):
            bias = jnp.where(owner == owner_ref[s, row], 0.0, bias)
        bias = jnp.broadcast_to(bias, (QUERY_BLOCK, devices * KEY_BLOCK)).astype(bf16)
        bias = jnp.concatenate([bias, causal[...]], axis=1)
        turned = keys.T
        blank = jnp.zeros((HEAD_DIM, key_count), bf16)
        wide_keys = jnp.concatenate(
            [
                jnp.concatenate([turned[:HEAD_DIM], blank, bias], axis=0),
                jnp.concatenate([blank, turned[HEAD_DIM:], bias], axis=0),
            ],
            axis=1,
        )
        wide_values = jnp.concatenate(
            [
                jnp.concatenate([values * low_mask, low_mask], axis=1),
                jnp.concatenate([values * high_mask, high_mask], axis=1),
            ],
            axis=0,
        )
        keys_now[...] = wide_keys
        values_now[...] = wide_values
        sections = [slice(m * QUERY_BLOCK, (m + 1) * QUERY_BLOCK) for m in range(slices)]
        for m, section in enumerate(sections):
            q = jnp.concatenate([queries[rows, m * LANES : (m + 1) * LANES], eye[...]], axis=1)
            scores[section, :] = jnp.dot(q, keys_now[...], preferred_element_type=f32)
        for section in sections:
            for side in range(2):
                cols = slice(side * key_count, (side + 1) * key_count)
                s = scores[section, cols]
                weights[section, cols] = jnp.exp(s - jnp.max(s, axis=1, keepdims=True)).astype(bf16)
        for m, section in enumerate(sections):
            mixed = jnp.dot(weights[section, :], values_now[...], preferred_element_type=f32)
            mix[rows, m * LANES : (m + 1) * LANES] = (mixed[:, :LANES] / mixed[:, LANES:]).astype(
                bf16
            )
        mix_copy(b).start()

    def part_of(left, right, rows, side, c):
        cols = pl.ds(pl.multiple_of(side * half + c * COLS, COLS), COLS)
        return jnp.dot(left[rows, :], right[:, cols], preferred_element_type=f32).astype(bf16)

    def ss_copy(b):
        return pltpu.make_async_remote_copy(
            src_ref=ss.at[b],
            dst_ref=ss_other.at[b],
            send_sem=ss_send.at[0],
            recv_sem=ss_recv.at[group_of(b)],
            device_id={"tp": other},
            device_id_type=MESH,
        )

    def squares(total, added):
        for k in range(COLS // LANES):
            piece = added[:, k * LANES : (k + 1) * LANES]
            total = total + piece * piece
        return total

    def project(first, count):
        wait_mix(first, count)
        size = count * QUERY_BLOCK
        rows = pl.ds(pl.multiple_of(first * QUERY_BLOCK, QUERY_BLOCK), size)
        total = jnp.zeros((size, LANES), f32)
        for c in range(half // COLS):
            mine = part_of(mix, ow, rows, core, c)
            theirs = part_of(mix_other, ow_other, rows, core, c)
            added = mine.astype(f32) + theirs.astype(f32)
            proj[rows, c * COLS : (c + 1) * COLS] = added
            total = squares(total, added)
        for j in range(count):
            ss[first + j] = total[j * QUERY_BLOCK : (j + 1) * QUERY_BLOCK]
            ss_copy(first + j).start()

    def normed(rows, total):
        scale = lax.rsqrt(jnp.sum(total, axis=1, keepdims=True) / (2 * half) + norm_eps)
        for c in range(half // LANES):
            at = slice(c * LANES, (c + 1) * LANES)
            out[rows, at] = (proj[rows, at] * scale * gain[:, at]).astype(bf16)

    def norm(first, count):
        landed = ss_other.at[pl.ds(first, count)]
        pltpu.make_async_copy(landed, landed, ss_recv.at[group_of(first)]).wait()

        @pl.loop(0, count)
        def _(j):
            b = first + j
            rows = pl.ds(pl.multiple_of(b * QUERY_BLOCK, QUERY_BLOCK), QUERY_BLOCK)
            normed(rows, ss[b] + ss_other[b])

    @pl.loop(0, qblocks)
    def _(b):
        attend(b)

        @pl.when(b == 1)
        def _():
            ow_copy.wait_recv()

        late = jnp.logical_and(b >= 2 * blocks_in, b % blocks_in == 0)

        @pl.when(jnp.logical_or(b == blocks_in - 1, late))
        def _():
            project(jnp.where(late, b - blocks_in, 0), blocks_in)

        @pl.when(late)
        def _():
            norm(b - 2 * blocks_in, blocks_in)

    project(last - 1, 1)
    norm(last - 1 - blocks_in, blocks_in)
    final = slice(last * QUERY_BLOCK, qblocks * QUERY_BLOCK)
    for n, side in enumerate((other, core)):
        for c in range(half // COLS):
            at = n * half + c * COLS
            partial[:, at : at + COLS] = part_of(mix, ow, final, side, c)

    @pl.loop(0, devices)
    def _(dst):
        @pl.when(dst > me)
        def _():
            sent = send.at[pl.ds(dst * qblocks, qblocks)]
            pltpu.make_async_copy(sent, sent, kv_send.at[dst]).wait()

    ow_copy.wait_send()
    pltpu.make_async_copy(ss.at[pl.ds(0, last)], ss.at[pl.ds(0, last)], ss_send.at[0]).wait()
    norm(last - 1, 1)
    wait_mix(last, 1)
    total = jnp.zeros((QUERY_BLOCK, LANES), f32)
    for n, side in enumerate((other, core)):
        for c in range(half // COLS):
            at = n * half + c * COLS
            theirs = part_of(mix_other, ow_other, final, side, c)
            added = partial[:, at : at + COLS].astype(f32) + theirs.astype(f32)
            if side is core:
                proj[final, c * COLS : (c + 1) * COLS] = added
            total = squares(total, added)
    normed(final, total)
    pltpu.make_async_copy(mix, mix, mix_send.at[0]).wait()


def store_kernel(held, out, sems):
    def copy(b):
        rows = pl.ds(b * QUERY_BLOCK, QUERY_BLOCK)
        return pltpu.make_async_copy(held.at[rows], out.at[rows], sems.at[b])

    for b in range(sems.shape[0]):
        copy(b).start()
    for b in range(sems.shape[0]):
        copy(b).wait()


def trig_table(blocks):
    half_dim = HEAD_DIM // 2
    lane = np.arange(LANES)
    frequency = (rope_base ** (-(lane % half_dim) / half_dim)).astype(np.float32)
    sign = np.where(lane % HEAD_DIM < half_dim, -1.0, 1.0)
    near = np.arange(QUERY_BLOCK)[:, None] * frequency.astype(np.float64)
    far = (np.arange(blocks)[:, None] * np.float32(QUERY_BLOCK) * frequency).astype(np.float64)
    parts = [np.cos(near), sign * np.sin(near), np.cos(far), sign * np.sin(far)]
    return np.concatenate(parts, axis=0).astype(np.float32)


def body(
    tokens, query_weight, key_weight, value_weight, out_weight, norm_gain, chosen_owner, chosen_part
):
    row_data = tokens[0]
    count = row_data.shape[0]
    devices = lax.axis_size("kv")
    qblocks = count // QUERY_BLOCK
    heads_width = query_weight.shape[1]
    half = norm_gain.shape[0]
    hbm = pl.BlockSpec(memory_space=pl.ANY)
    vmem = pl.BlockSpec(memory_space=pltpu.VMEM)
    bf16, f32 = jnp.bfloat16, jnp.float32
    slots = chosen_owner.shape[1:][::-1]
    key_count = devices * KEY_BLOCK + QUERY_BLOCK
    trig = trig_table(devices * qblocks)
    operands = [
        chosen_owner[0].T, chosen_part[0].T, row_data, query_weight, key_weight, value_weight,
        out_weight, norm_gain[None], jnp.asarray(trig),
    ]
    operands = [pltpu.with_memory_space_constraint(x, pltpu.HBM) for x in operands]
    result = pl.pallas_call(
        functools.partial(kernel, devices),
        out_shape=pltpu.VMEM((count, half), bf16),
        in_specs=[hbm] * len(operands),
        out_specs=vmem,
        scratch_shapes=[
            pltpu.SMEM(slots, jnp.int32),
            pltpu.SMEM(slots, jnp.int32),
            pltpu.VMEM((1, half), f32),
            pltpu.VMEM(trig.shape, f32),
            pltpu.SemaphoreType.DMA((4,)),
            pltpu.VMEM((count, LANES), f32),
            pltpu.VMEM((count, LANES), f32),
            pltpu.VMEM((QUERY_BLOCK, QUERY_BLOCK), bf16),
            pltpu.VMEM((QUERY_BLOCK, QUERY_BLOCK), bf16),
            pltpu.VMEM(row_data.shape, bf16),
            pltpu.VMEM(query_weight.shape, bf16),
            pltpu.VMEM((key_weight.shape[0], 2 * key_weight.shape[1]), bf16),
            pltpu.VMEM(out_weight.shape, bf16),
            pltpu.SemaphoreType.DMA((2,)),
            pltpu.SemaphoreType.DMA((3,)),
            pltpu.VMEM((count // KEY_BLOCK, KEY_BLOCK, 2 * LANES), bf16),
            pltpu.VMEM((devices * qblocks, KEY_BLOCK, 2 * LANES), bf16),
            pltpu.VMEM((devices * qblocks, KEY_BLOCK, 2 * LANES), bf16),
            pltpu.VMEM((count, heads_width), bf16),
            pltpu.VMEM((LANES + QUERY_BLOCK, 2 * key_count), bf16),
            pltpu.VMEM((2 * key_count, 2 * LANES), bf16),
            pltpu.VMEM((heads_width // LANES * QUERY_BLOCK, 2 * key_count), f32),
            pltpu.VMEM((heads_width // LANES * QUERY_BLOCK, 2 * key_count), bf16),
            pltpu.VMEM((count, heads_width), bf16),
            pltpu.VMEM((count, heads_width), bf16),
            pltpu.VMEM(out_weight.shape, bf16),
            pltpu.VMEM((QUERY_BLOCK, 2 * half), bf16),
            pltpu.VMEM((count, half), f32),
            pltpu.VMEM((qblocks, QUERY_BLOCK, LANES), f32),
            pltpu.VMEM((qblocks, QUERY_BLOCK, LANES), f32),
            pltpu.SemaphoreType.DMA((devices,)),
            pltpu.SemaphoreType.DMA((qblocks,)),
            pltpu.SemaphoreType.DMA((2,)),
            pltpu.SemaphoreType.DMA((1,)),
            pltpu.SemaphoreType.DMA((count // ROWS + 1,)),
            pltpu.SemaphoreType.DMA((1,)),
            pltpu.SemaphoreType.DMA((count // ROWS,)),
        ],
        compiler_params=pltpu.CompilerParams(
            collective_id=0, has_side_effects=True, vmem_limit_bytes=48 * 1024 * 1024
        ),
    )(*operands)
    return pl.pallas_call(
        store_kernel,
        out_shape=jax.ShapeDtypeStruct((count, half), bf16),
        in_specs=[vmem],
        out_specs=hbm,
        scratch_shapes=[pltpu.SemaphoreType.DMA((qblocks,))],
        compiler_params=pltpu.CompilerParams(vmem_limit_bytes=4 * 1024 * 1024),
    )(pltpu.with_memory_space_constraint(result, pltpu.VMEM))[None]


def solution(mesh):
    placed = (
        P("dp", "kv", None),
        P(None, "tp"),
        P(None, "tp"),
        P(None, "tp"),
        P("tp", None),
        P("tp"),
        P("dp", None, None),
        P("dp", None, None),
    )
    return jax.shard_map(
        body, mesh=mesh, in_specs=placed, out_specs=P("dp", "kv", "tp"), check_vma=False
    )
```

```python
import functools

import jax
import jax.numpy as jnp
import numpy as np
from jax import lax
from jax.experimental import pallas as pl
from jax.experimental.pallas import tpu as pltpu
from jax.sharding import PartitionSpec as P

HEAD_DIM = 64
QUERY_BLOCK = 128
KEY_BLOCK = 64
LANES = 128
ROWS = 256
COLS = 256

rope_base = 10000.0
norm_eps = 1e-06
hidden = -1e38
MESH = pl.DeviceIdType.MESH


def low_lanes(shape):
    return lax.broadcasted_iota(jnp.int32, shape, 1) < HEAD_DIM


def turn(u, cosine, sine):
    lane = lax.broadcasted_iota(jnp.int32, u.shape, 1)
    half = HEAD_DIM // 2
    swapped = jnp.where(
        lane % HEAD_DIM < half, pltpu.roll(u, LANES - half, 1), pltpu.roll(u, half, 1)
    )
    return u * cosine + swapped * sine


def kernel(
    devices, owner_hbm, part_hbm, tok_hbm, wq_hbm, wk_hbm, wv_hbm, ow_hbm, gain_hbm, trig_hbm, out,
    owner_ref, part_ref, gain, trig, small_sems, cosine, sine, eye, causal,
    tok, wq, wkv, ow, tok_sems, weight_sems,
    kv, send, pool, queries, keys_now, values_now, scores, weights, mix, mix_other, ow_other, partial, proj, ss, ss_other,
    kv_send, kv_recv, ow_sems, mix_send, mix_recv, ss_send, ss_recv,
):
    me = lax.axis_index("kv")
    core = lax.axis_index("tp")
    other = 1 - core
    tokens = tok.shape[0]
    qblocks = tokens // QUERY_BLOCK
    chosen = owner_ref.shape[0]
    half = gain.shape[1]
    row_steps = tokens // ROWS
    per_q = QUERY_BLOCK // KEY_BLOCK
    key_width = wk_hbm.shape[1]
    slices = wq.shape[1] // LANES
    heads = wq.shape[1] // HEAD_DIM
    bf16, f32 = jnp.bfloat16, jnp.float32

    part_rows = tokens // 2

    def tok_copy(r):
        rows = pl.ds(pl.multiple_of(r * part_rows, part_rows), part_rows)
        return pltpu.make_async_copy(tok_hbm.at[rows], tok.at[rows], tok_sems.at[r])

    wk_copy = pltpu.make_async_copy(wk_hbm, wkv.at[:, pl.ds(0, key_width)], weight_sems.at[0])
    wv_copy = pltpu.make_async_copy(
        wv_hbm, wkv.at[:, pl.ds(key_width, key_width)], weight_sems.at[0]
    )
    wq_copy = pltpu.make_async_copy(wq_hbm, wq, weight_sems.at[1])
    ow_loads = []
    for m in range(slices):
        for g in range(2):
            ow_loads.append(
                pltpu.make_async_copy(
                    ow_hbm.at[pl.ds((g * slices + m) * HEAD_DIM, HEAD_DIM)],
                    ow.at[pl.ds((2 * m + g) * HEAD_DIM, HEAD_DIM)],
                    weight_sems.at[2],
                )
            )
    small = [
        pltpu.make_async_copy(trig_hbm, trig, small_sems.at[0]),
        pltpu.make_async_copy(owner_hbm, owner_ref, small_sems.at[1]),
        pltpu.make_async_copy(part_hbm, part_ref, small_sems.at[2]),
        pltpu.make_async_copy(gain_hbm, gain, small_sems.at[3]),
    ]
    small[0].start()
    wk_copy.start()
    wv_copy.start()
    tok_copy(0).start()
    tok_copy(1).start(priority=1)
    for copy in small[1:]:
        copy.start(priority=1)

    barrier = pltpu.get_barrier_semaphore()

    @pl.loop(0, devices)
    def _(j):
        @pl.when(j != me)
        def _():
            pl.semaphore_signal(barrier, inc=1, device_id={"kv": j}, device_id_type=MESH)

    pl.semaphore_signal(barrier, inc=1, device_id={"tp": other}, device_id_type=MESH)

    square = (QUERY_BLOCK, QUERY_BLOCK)
    first = lax.broadcasted_iota(jnp.int32, square, 0)
    second = lax.broadcasted_iota(jnp.int32, square, 1)
    eye[...] = jnp.where(first == second, 1.0, 0.0).astype(bf16)
    causal[...] = jnp.where(first >= second, 0.0, hidden).astype(bf16)

    small[0].wait()
    near_cos = trig[0:QUERY_BLOCK, :]
    near_sin = trig[QUERY_BLOCK : 2 * QUERY_BLOCK, :]

    @pl.loop(0, qblocks)
    def _(b):
        rows = pl.ds(pl.multiple_of(b * QUERY_BLOCK, QUERY_BLOCK), QUERY_BLOCK)
        at = 2 * QUERY_BLOCK + me * qblocks + b
        far_cos = trig[pl.ds(at, 1), :]
        far_sin = trig[pl.ds(at + devices * qblocks, 1), :]
        cosine[rows, :] = far_cos * near_cos - far_sin * near_sin
        sine[rows, :] = far_sin * near_cos + far_cos * near_sin

    pltpu.make_async_copy(wkv, wkv, weight_sems.at[0]).wait()

    @pl.loop(0, 2)
    def _(r):
        tok_copy(r).wait()

        @pl.when(r == 0)
        def _():
            wq_copy.start(priority=1)
            for copy in ow_loads:
                copy.start(priority=1)

        rows = pl.ds(pl.multiple_of(r * part_rows, part_rows), part_rows)
        both = jnp.dot(tok[rows, :], wkv[...], preferred_element_type=f32)
        keys = turn(both[:, :LANES], cosine[rows, :], sine[rows, :])
        joined = jnp.concatenate([keys, both[:, LANES:]], axis=1).astype(bf16)
        blocks = part_rows // KEY_BLOCK
        kv[pl.ds(r * blocks, blocks)] = joined.reshape(blocks, KEY_BLOCK, 2 * LANES)

    for copy in small[1:]:
        copy.wait()
    pl.semaphore_wait(barrier, devices)

    def place(src, row, s):
        return owner_ref[s, row] == src, part_ref[s, row]

    def wanted(dst, q):
        found = [place(me, dst * qblocks + q, s) for s in range(chosen)]
        return sum(jnp.where(here, at, 0) for here, at in found)

    def kv_copy(dst, q, lanes, sem):
        return pltpu.make_async_remote_copy(
            src_ref=send.at[pl.ds(dst * qblocks + q, 1), :, lanes],
            dst_ref=pool.at[pl.ds(q * devices + me, 1), :, lanes],
            send_sem=kv_send.at[dst],
            recv_sem=kv_recv.at[sem],
            device_id={"kv": dst},
            device_id_type=MESH,
        )

    last = qblocks - 1
    all_lanes, key_lanes, value_lanes = (
        pl.ds(0, 2 * LANES), pl.ds(0, LANES), pl.ds(LANES, LANES)
    )

    def send_block(q, split):
        @pl.loop(0, devices - 1)
        def _(step):
            dst = devices - 1 - step

            @pl.when(dst > me)
            def _():
                send[pl.ds(dst * qblocks + q, 1)] = kv[pl.ds(wanted(dst, q), 1)]
                kv_copy(dst, q, key_lanes if split else all_lanes, q).start()

        if split:

            @pl.loop(0, devices - 1)
            def _(step):
                dst = devices - 1 - step

                @pl.when(dst > me)
                def _():
                    kv_copy(dst, q, value_lanes, qblocks).start()

    paced = me + 3 < devices

    @pl.loop(0, jnp.where(paced, 1, last))
    def _(q):
        send_block(q, False)

    @pl.when(jnp.logical_not(paced))
    def _():
        send_block(last, True)

    @pl.loop(0, qblocks)
    def _(q):
        pool[pl.ds(q * devices + me, 1)] = kv[pl.ds(wanted(me, q), 1)]

        @pl.loop(0, devices)
        def _(src):
            @pl.when(src > me)
            def _():
                pool[pl.ds(q * devices + src, 1)] = jnp.zeros((1, KEY_BLOCK, 2 * LANES), bf16)

    ow_copy = pltpu.make_async_remote_copy(
        src_ref=ow,
        dst_ref=ow_other,
        send_sem=ow_sems.at[0],
        recv_sem=ow_sems.at[1],
        device_id={"tp": other},
        device_id_type=MESH,
    )
    wq_copy.wait()

    @pl.loop(0, row_steps)
    def _(r):
        @pl.when(jnp.logical_and(paced, r == row_steps - 1))
        def _():
            send_block(1, False)

        @pl.when(r == 1)
        def _():
            pltpu.make_async_copy(ow, ow, weight_sems.at[2]).wait()
            ow_copy.start()

        rows = pl.ds(pl.multiple_of(r * ROWS, ROWS), ROWS)
        scale = HEAD_DIM**-0.5
        scaled_cos, scaled_sin = cosine[rows, :] * scale, sine[rows, :] * scale
        for c in range(wq.shape[1] // COLS):
            part = jnp.dot(
                tok[rows, :], wq[:, c * COLS : (c + 1) * COLS], preferred_element_type=f32
            )
            for k in range(COLS // LANES):
                turned = turn(part[:, k * LANES : (k + 1) * LANES], scaled_cos, scaled_sin)
                away = pltpu.roll(turned, HEAD_DIM, 1)
                for j in range(2):
                    head = 2 * (c * (COLS // LANES) + k) + j
                    group, m = head // slices, head % slices
                    lanes = slice(group * HEAD_DIM, (group + 1) * HEAD_DIM)
                    at = m * LANES + group * HEAD_DIM
                    queries[rows, at : at + HEAD_DIM] = (
                        turned if group == j else away
                    )[:, lanes].astype(bf16)

    key_count = devices * KEY_BLOCK + QUERY_BLOCK

    blocks_in = ROWS // QUERY_BLOCK

    def group_of(b):
        return b // blocks_in + jnp.where(b == last, 1, 0)

    def wait_mix(first, count):
        rows = pl.ds(pl.multiple_of(first * QUERY_BLOCK, QUERY_BLOCK), count * QUERY_BLOCK)
        landed = mix_other.at[rows]
        pltpu.make_async_copy(landed, landed, mix_recv.at[group_of(first)]).wait()

    def mix_copy(b):
        rows = pl.ds(pl.multiple_of(b * QUERY_BLOCK, QUERY_BLOCK), QUERY_BLOCK)
        return pltpu.make_async_remote_copy(
            src_ref=mix.at[rows],
            dst_ref=mix_other.at[rows],
            send_sem=mix_send.at[0],
            recv_sem=mix_recv.at[group_of(b)],
            device_id={"tp": other},
            device_id_type=MESH,
        )

    low_mask = jnp.where(low_lanes((key_count, LANES)), 1.0, 0.0).astype(bf16)
    high_mask = jnp.where(low_lanes((key_count, LANES)), 0.0, 1.0).astype(bf16)

    def wait_kv(b, lanes, sem):
        for n in range(1, devices):

            @pl.when(me == n)
            def _():
                landed = pool.at[pl.ds(b * devices, n), :, lanes]
                pltpu.make_async_copy(landed, landed, kv_recv.at[sem]).wait()

    def block_of(b, lanes):
        far = pool[pl.ds(b * devices, devices), :, lanes].reshape(devices * KEY_BLOCK, LANES)
        near = kv[pl.ds(b * per_q, per_q), :, lanes].reshape(QUERY_BLOCK, LANES)
        return jnp.concatenate([far, near], axis=0)

    sections = [slice(m * QUERY_BLOCK, (m + 1) * QUERY_BLOCK) for m in range(slices)]

    def attend_keys(b):
        row = me * qblocks + b
        rows = pl.ds(pl.multiple_of(b * QUERY_BLOCK, QUERY_BLOCK), QUERY_BLOCK)
        keys = block_of(b, slice(0, LANES))
        owner = lax.broadcasted_iota(jnp.int32, (1, devices * KEY_BLOCK), 1) // KEY_BLOCK
        bias = jnp.full((1, devices * KEY_BLOCK), hidden, f32)
        for s in range(chosen):
            bias = jnp.where(owner == owner_ref[s, row], 0.0, bias)
        bias = jnp.broadcast_to(bias, (QUERY_BLOCK, devices * KEY_BLOCK)).astype(bf16)
        bias = jnp.concatenate([bias, causal[...]], axis=1)
        turned = keys.T
        blank = jnp.zeros((HEAD_DIM, key_count), bf16)
        wide_keys = jnp.concatenate(
            [
                jnp.concatenate([turned[:HEAD_DIM], blank, bias], axis=0),
                jnp.concatenate([blank, turned[HEAD_DIM:], bias], axis=0),
            ],
            axis=1,
        )
        keys_now[...] = wide_keys
        for m, section in enumerate(sections):
            q = jnp.concatenate([queries[rows, m * LANES : (m + 1) * LANES], eye[...]], axis=1)
            scores[section, :] = jnp.dot(q, keys_now[...], preferred_element_type=f32)
        for section in sections:
            for side in range(2):
                cols = slice(side * key_count, (side + 1) * key_count)
                s = scores[section, cols]
                weights[section, cols] = jnp.exp(s - jnp.max(s, axis=1, keepdims=True)).astype(bf16)

    def attend_values(b):
        rows = pl.ds(pl.multiple_of(b * QUERY_BLOCK, QUERY_BLOCK), QUERY_BLOCK)
        values = block_of(b, slice(LANES, 2 * LANES))
        values_now[...] = jnp.concatenate(
            [
                jnp.concatenate([values * low_mask, low_mask], axis=1),
                jnp.concatenate([values * high_mask, high_mask], axis=1),
            ],
            axis=0,
        )
        for m, section in enumerate(sections):
            mixed = jnp.dot(weights[section, :], values_now[...], preferred_element_type=f32)
            mix[rows, m * LANES : (m + 1) * LANES] = (mixed[:, :LANES] / mixed[:, LANES:]).astype(
                bf16
            )
        mix_copy(b).start()

    def part_of(left, right, rows, side, c):
        cols = pl.ds(pl.multiple_of(side * half + c * COLS, COLS), COLS)
        return jnp.dot(left[rows, :], right[:, cols], preferred_element_type=f32).astype(bf16)

    def ss_copy(b):
        return pltpu.make_async_remote_copy(
            src_ref=ss.at[b],
            dst_ref=ss_other.at[b],
            send_sem=ss_send.at[0],
            recv_sem=ss_recv.at[group_of(b)],
            device_id={"tp": other},
            device_id_type=MESH,
        )

    def squares(total, added):
        for k in range(COLS // LANES):
            piece = added[:, k * LANES : (k + 1) * LANES]
            total = total + piece * piece
        return total

    def project(first, count):
        wait_mix(first, count)
        size = count * QUERY_BLOCK
        rows = pl.ds(pl.multiple_of(first * QUERY_BLOCK, QUERY_BLOCK), size)
        total = jnp.zeros((size, LANES), f32)
        for c in range(half // COLS):
            mine = part_of(mix, ow, rows, core, c)
            theirs = part_of(mix_other, ow_other, rows, core, c)
            added = mine.astype(f32) + theirs.astype(f32)
            proj[rows, c * COLS : (c + 1) * COLS] = added
            total = squares(total, added)
        for j in range(count):
            ss[first + j] = total[j * QUERY_BLOCK : (j + 1) * QUERY_BLOCK]
            ss_copy(first + j).start()

    def normed(rows, total):
        scale = lax.rsqrt(jnp.sum(total, axis=1, keepdims=True) / (2 * half) + norm_eps)
        for c in range(half // LANES):
            at = slice(c * LANES, (c + 1) * LANES)
            out[rows, at] = (proj[rows, at] * scale * gain[:, at]).astype(bf16)

    def norm(first, count):
        landed = ss_other.at[pl.ds(first, count)]
        pltpu.make_async_copy(landed, landed, ss_recv.at[group_of(first)]).wait()

        @pl.loop(0, count)
        def _(j):
            b = first + j
            rows = pl.ds(pl.multiple_of(b * QUERY_BLOCK, QUERY_BLOCK), QUERY_BLOCK)
            normed(rows, ss[b] + ss_other[b])

    @pl.loop(0, last)
    def _(b):
        wait_kv(b, all_lanes, b)
        attend_keys(b)
        attend_values(b)

        @pl.when(b == 1)
        def _():
            ow_copy.wait_recv()

        @pl.when(jnp.logical_and(paced, jnp.logical_and(b > 0, b < last - 2)))
        def _():
            send_block(b + 1, False)

        @pl.when(b % blocks_in == blocks_in - 1)
        def _():
            project(b + 1 - blocks_in, blocks_in)

        @pl.when(jnp.logical_and(paced, b == last - 2))
        def _():
            send_block(last - 1, False)

        @pl.when(jnp.logical_and(b > 0, b % blocks_in == 0))
        def _():
            norm(b - blocks_in, blocks_in)

    @pl.when(paced)
    def _():
        send_block(last, True)

    project(last - 1, 1)
    wait_kv(last, key_lanes, last)
    attend_keys(last)
    wait_kv(last, value_lanes, qblocks)
    attend_values(last)
    final = slice(last * QUERY_BLOCK, qblocks * QUERY_BLOCK)
    for n, side in enumerate((other, core)):
        for c in range(half // COLS):
            at = n * half + c * COLS
            partial[:, at : at + COLS] = part_of(mix, ow, final, side, c)

    @pl.loop(0, devices)
    def _(dst):
        @pl.when(dst > me)
        def _():
            sent = send.at[pl.ds(dst * qblocks, qblocks)]
            pltpu.make_async_copy(sent, sent, kv_send.at[dst]).wait()

    ow_copy.wait_send()
    pltpu.make_async_copy(ss.at[pl.ds(0, last)], ss.at[pl.ds(0, last)], ss_send.at[0]).wait()
    norm(last - 1, 1)
    wait_mix(last, 1)
    total = jnp.zeros((QUERY_BLOCK, LANES), f32)
    for n, side in enumerate((other, core)):
        for c in range(half // COLS):
            at = n * half + c * COLS
            theirs = part_of(mix_other, ow_other, final, side, c)
            added = partial[:, at : at + COLS].astype(f32) + theirs.astype(f32)
            if side is core:
                proj[final, c * COLS : (c + 1) * COLS] = added
            total = squares(total, added)
    normed(final, total)
    pltpu.make_async_copy(mix, mix, mix_send.at[0]).wait()


def store_kernel(held, out, sems):
    def copy(b):
        rows = pl.ds(b * QUERY_BLOCK, QUERY_BLOCK)
        return pltpu.make_async_copy(held.at[rows], out.at[rows], sems.at[b])

    for b in range(sems.shape[0]):
        copy(b).start()
    for b in range(sems.shape[0]):
        copy(b).wait()


def trig_table(blocks):
    half_dim = HEAD_DIM // 2
    lane = np.arange(LANES)
    frequency = (rope_base ** (-(lane % half_dim) / half_dim)).astype(np.float32)
    sign = np.where(lane % HEAD_DIM < half_dim, -1.0, 1.0)
    near = np.arange(QUERY_BLOCK)[:, None] * frequency.astype(np.float64)
    far = (np.arange(blocks)[:, None] * np.float32(QUERY_BLOCK) * frequency).astype(np.float64)
    parts = [np.cos(near), sign * np.sin(near), np.cos(far), sign * np.sin(far)]
    return np.concatenate(parts, axis=0).astype(np.float32)


def body(
    tokens, query_weight, key_weight, value_weight, out_weight, norm_gain, chosen_owner, chosen_part
):
    row_data = tokens[0]
    count = row_data.shape[0]
    devices = lax.axis_size("kv")
    qblocks = count // QUERY_BLOCK
    heads_width = query_weight.shape[1]
    half = norm_gain.shape[0]
    hbm = pl.BlockSpec(memory_space=pl.ANY)
    vmem = pl.BlockSpec(memory_space=pltpu.VMEM)
    bf16, f32 = jnp.bfloat16, jnp.float32
    slots = chosen_owner.shape[1:][::-1]
    key_count = devices * KEY_BLOCK + QUERY_BLOCK
    trig = trig_table(devices * qblocks)
    operands = [
        chosen_owner[0].T, chosen_part[0].T, row_data, query_weight, key_weight, value_weight,
        out_weight, norm_gain[None], jnp.asarray(trig),
    ]
    operands = [pltpu.with_memory_space_constraint(x, pltpu.HBM) for x in operands]
    result = pl.pallas_call(
        functools.partial(kernel, devices),
        out_shape=pltpu.VMEM((count, half), bf16),
        in_specs=[hbm] * len(operands),
        out_specs=vmem,
        scratch_shapes=[
            pltpu.SMEM(slots, jnp.int32),
            pltpu.SMEM(slots, jnp.int32),
            pltpu.VMEM((1, half), f32),
            pltpu.VMEM(trig.shape, f32),
            pltpu.SemaphoreType.DMA((4,)),
            pltpu.VMEM((count, LANES), f32),
            pltpu.VMEM((count, LANES), f32),
            pltpu.VMEM((QUERY_BLOCK, QUERY_BLOCK), bf16),
            pltpu.VMEM((QUERY_BLOCK, QUERY_BLOCK), bf16),
            pltpu.VMEM(row_data.shape, bf16),
            pltpu.VMEM(query_weight.shape, bf16),
            pltpu.VMEM((key_weight.shape[0], 2 * key_weight.shape[1]), bf16),
            pltpu.VMEM(out_weight.shape, bf16),
            pltpu.SemaphoreType.DMA((2,)),
            pltpu.SemaphoreType.DMA((3,)),
            pltpu.VMEM((count // KEY_BLOCK, KEY_BLOCK, 2 * LANES), bf16),
            pltpu.VMEM((devices * qblocks, KEY_BLOCK, 2 * LANES), bf16),
            pltpu.VMEM((devices * qblocks, KEY_BLOCK, 2 * LANES), bf16),
            pltpu.VMEM((count, heads_width), bf16),
            pltpu.VMEM((LANES + QUERY_BLOCK, 2 * key_count), bf16),
            pltpu.VMEM((2 * key_count, 2 * LANES), bf16),
            pltpu.VMEM((heads_width // LANES * QUERY_BLOCK, 2 * key_count), f32),
            pltpu.VMEM((heads_width // LANES * QUERY_BLOCK, 2 * key_count), bf16),
            pltpu.VMEM((count, heads_width), bf16),
            pltpu.VMEM((count, heads_width), bf16),
            pltpu.VMEM(out_weight.shape, bf16),
            pltpu.VMEM((QUERY_BLOCK, 2 * half), bf16),
            pltpu.VMEM((count, half), f32),
            pltpu.VMEM((qblocks, QUERY_BLOCK, LANES), f32),
            pltpu.VMEM((qblocks, QUERY_BLOCK, LANES), f32),
            pltpu.SemaphoreType.DMA((devices,)),
            pltpu.SemaphoreType.DMA((qblocks + 1,)),
            pltpu.SemaphoreType.DMA((2,)),
            pltpu.SemaphoreType.DMA((1,)),
            pltpu.SemaphoreType.DMA((count // ROWS + 1,)),
            pltpu.SemaphoreType.DMA((1,)),
            pltpu.SemaphoreType.DMA((count // ROWS,)),
        ],
        compiler_params=pltpu.CompilerParams(
            collective_id=0, has_side_effects=True, vmem_limit_bytes=48 * 1024 * 1024
        ),
    )(*operands)
    return pl.pallas_call(
        store_kernel,
        out_shape=jax.ShapeDtypeStruct((count, half), bf16),
        in_specs=[vmem],
        out_specs=hbm,
        scratch_shapes=[pltpu.SemaphoreType.DMA((qblocks,))],
        compiler_params=pltpu.CompilerParams(vmem_limit_bytes=4 * 1024 * 1024),
    )(pltpu.with_memory_space_constraint(result, pltpu.VMEM))[None]


def solution(mesh):
    placed = (
        P("dp", "kv", None),
        P(None, "tp"),
        P(None, "tp"),
        P(None, "tp"),
        P("tp", None),
        P("tp"),
        P("dp", None, None),
        P("dp", None, None),
    )
    return jax.shard_map(
        body, mesh=mesh, in_specs=placed, out_specs=P("dp", "kv", "tp"), check_vma=False
    )
```

```python
import functools

import jax
import jax.numpy as jnp
import numpy as np
from jax import lax
from jax.experimental import pallas as pl
from jax.experimental.pallas import tpu as pltpu
from jax.sharding import PartitionSpec as P

HEAD_DIM = 64
QUERY_BLOCK = 128
KEY_BLOCK = 64
LANES = 128
ROWS = 256
COLS = 256

rope_base = 10000.0
norm_eps = 1e-06
hidden = -1e38
MESH = pl.DeviceIdType.MESH


def low_lanes(shape):
    return lax.broadcasted_iota(jnp.int32, shape, 1) < HEAD_DIM


def turn(u, cosine, sine):
    lane = lax.broadcasted_iota(jnp.int32, u.shape, 1)
    half = HEAD_DIM // 2
    swapped = jnp.where(
        lane % HEAD_DIM < half, pltpu.roll(u, LANES - half, 1), pltpu.roll(u, half, 1)
    )
    return u * cosine + swapped * sine


def part_of(left, right, rows, half, side, c):
    cols = pl.ds(pl.multiple_of(side * half + c * COLS, COLS), COLS)
    return jnp.dot(
        left[rows, :], right[:, cols], preferred_element_type=jnp.float32
    ).astype(jnp.bfloat16)


def squares(total, added):
    for k in range(COLS // LANES):
        piece = added[:, k * LANES : (k + 1) * LANES]
        total = total + piece * piece
    return total


def row_scale(total, half):
    return lax.rsqrt(jnp.sum(total, axis=1, keepdims=True) / (2 * half) + norm_eps)


def kernel(
    devices, owner_hbm, part_hbm, tok_hbm, wq_hbm, wk_hbm, wv_hbm, ow_hbm, gain_hbm, near_hbm, far_hbm, out, mix_end, ow_other, partial, gain_end,
    owner_ref, part_ref, gain, near_trig, far_trig, small_sems, cosine, sine, eye, causal,
    tok, wq, wkv, ow, tok_sems, weight_sems,
    kv, send, pool, queries, keys_now, values_now, scores, weights, mix, mix_other, early, proj, ss, ss_other,
    kv_send, kv_recv, ow_sems, mix_send, mix_recv, ss_send, ss_recv,
):
    me = lax.axis_index("kv")
    core = lax.axis_index("tp")
    other = 1 - core
    tokens = tok.shape[0]
    qblocks = tokens // QUERY_BLOCK
    chosen = owner_ref.shape[0]
    half = gain.shape[1]
    row_steps = tokens // ROWS
    per_q = QUERY_BLOCK // KEY_BLOCK
    key_width = wk_hbm.shape[1]
    slices = wq.shape[1] // LANES
    heads = wq.shape[1] // HEAD_DIM
    bf16, f32 = jnp.bfloat16, jnp.float32

    pieces = ((0, ROWS), (ROWS, tokens - ROWS))

    def tok_copy(r):
        rows = pl.ds(*pieces[r])
        return pltpu.make_async_copy(tok_hbm.at[rows], tok.at[rows], tok_sems.at[r])

    wk_copy = pltpu.make_async_copy(wk_hbm, wkv.at[:, pl.ds(0, key_width)], weight_sems.at[0])
    wv_copy = pltpu.make_async_copy(
        wv_hbm, wkv.at[:, pl.ds(key_width, key_width)], weight_sems.at[0]
    )
    wq_copy = pltpu.make_async_copy(wq_hbm, wq, weight_sems.at[1])
    ow_loads = []
    for m in range(slices):
        for g in range(2):
            ow_loads.append(
                pltpu.make_async_copy(
                    ow_hbm.at[pl.ds((g * slices + m) * HEAD_DIM, HEAD_DIM)],
                    ow.at[pl.ds((2 * m + g) * HEAD_DIM, HEAD_DIM)],
                    weight_sems.at[2],
                )
            )
    small = [
        pltpu.make_async_copy(near_hbm, near_trig, small_sems.at[0]),
        pltpu.make_async_copy(far_hbm.at[me], far_trig, small_sems.at[4]),
        pltpu.make_async_copy(owner_hbm, owner_ref, small_sems.at[1]),
        pltpu.make_async_copy(part_hbm, part_ref, small_sems.at[2]),
        pltpu.make_async_copy(gain_hbm, gain, small_sems.at[3]),
    ]
    small[0].start()
    small[1].start()
    wk_copy.start()
    wv_copy.start()
    tok_copy(0).start()
    tok_copy(1).start(priority=1)
    for copy in small[2:]:
        copy.start(priority=1)

    barrier = pltpu.get_barrier_semaphore()

    @pl.loop(0, devices)
    def _(j):
        @pl.when(j != me)
        def _():
            pl.semaphore_signal(barrier, inc=1, device_id={"kv": j}, device_id_type=MESH)

    pl.semaphore_signal(barrier, inc=1, device_id={"tp": other}, device_id_type=MESH)

    square = (QUERY_BLOCK, QUERY_BLOCK)
    first = lax.broadcasted_iota(jnp.int32, square, 0)
    second = lax.broadcasted_iota(jnp.int32, square, 1)
    eye[...] = jnp.where(first == second, 1.0, 0.0).astype(bf16)
    causal[...] = jnp.where(first >= second, 0.0, hidden).astype(bf16)

    small[0].wait()
    small[1].wait()
    near_cos = near_trig[0:QUERY_BLOCK, :]
    near_sin = near_trig[QUERY_BLOCK : 2 * QUERY_BLOCK, :]

    @pl.loop(0, qblocks)
    def _(b):
        rows = pl.ds(pl.multiple_of(b * QUERY_BLOCK, QUERY_BLOCK), QUERY_BLOCK)
        far_cos = far_trig[pl.ds(b, 1), :]
        far_sin = far_trig[pl.ds(b + qblocks, 1), :]
        cosine[rows, :] = far_cos * near_cos - far_sin * near_sin
        sine[rows, :] = far_sin * near_cos + far_cos * near_sin

    pltpu.make_async_copy(wkv, wkv, weight_sems.at[0]).wait()

    once = jnp.where(core >= 0, 1, 0)
    for r, (start, size) in enumerate(pieces):

        @pl.loop(0, once)
        def _(_):
            tok_copy(r).wait()
            if r == 0:
                wq_copy.start(priority=1)
                for copy in ow_loads:
                    copy.start(priority=1)
            rows = pl.ds(start, size)
            both = jnp.dot(tok[rows, :], wkv[...], preferred_element_type=f32)
            keys = turn(both[:, :LANES], cosine[rows, :], sine[rows, :])
            joined = jnp.concatenate([keys, both[:, LANES:]], axis=1).astype(bf16)
            blocks = size // KEY_BLOCK
            kv[pl.ds(start // KEY_BLOCK, blocks)] = joined.reshape(blocks, KEY_BLOCK, 2 * LANES)

    for copy in small[2:]:
        copy.wait()
    pl.semaphore_wait(barrier, devices)

    def place(src, row, s):
        return owner_ref[s, row] == src, part_ref[s, row]

    def wanted(dst, q):
        found = [place(me, dst * qblocks + q, s) for s in range(chosen)]
        return sum(jnp.where(here, at, 0) for here, at in found)

    def kv_copy(dst, q, lanes, sem):
        return pltpu.make_async_remote_copy(
            src_ref=send.at[pl.ds(dst * qblocks + q, 1), :, lanes],
            dst_ref=pool.at[pl.ds(q * devices + me, 1), :, lanes],
            send_sem=kv_send.at[dst],
            recv_sem=kv_recv.at[sem],
            device_id={"kv": dst},
            device_id_type=MESH,
        )

    last = qblocks - 1
    all_lanes, key_lanes, value_lanes = (
        pl.ds(0, 2 * LANES), pl.ds(0, LANES), pl.ds(LANES, LANES)
    )

    def send_block(q, split):
        @pl.loop(0, devices - 1)
        def _(step):
            dst = devices - 1 - step

            @pl.when(dst > me)
            def _():
                send[pl.ds(dst * qblocks + q, 1)] = kv[pl.ds(wanted(dst, q), 1)]
                kv_copy(dst, q, key_lanes if split else all_lanes, q).start()

        if split:

            @pl.loop(0, devices - 1)
            def _(step):
                dst = devices - 1 - step

                @pl.when(dst > me)
                def _():
                    kv_copy(dst, q, value_lanes, qblocks).start()

    paced = me + 3 < devices

    @pl.loop(0, jnp.where(paced, 1, last))
    def _(q):
        send_block(q, False)

    @pl.when(jnp.logical_not(paced))
    def _():
        send_block(last, True)

    @pl.loop(0, qblocks)
    def _(q):
        pool[pl.ds(q * devices + me, 1)] = kv[pl.ds(wanted(me, q), 1)]

        @pl.loop(0, devices)
        def _(src):
            @pl.when(src > me)
            def _():
                pool[pl.ds(q * devices + src, 1)] = jnp.zeros((1, KEY_BLOCK, 2 * LANES), bf16)

    ow_copy = pltpu.make_async_remote_copy(
        src_ref=ow,
        dst_ref=ow_other,
        send_sem=ow_sems.at[0],
        recv_sem=ow_sems.at[1],
        device_id={"tp": other},
        device_id_type=MESH,
    )
    wq_copy.wait()

    @pl.loop(0, row_steps)
    def _(r):
        @pl.when(jnp.logical_and(paced, r == row_steps - 1))
        def _():
            send_block(1, False)

        @pl.when(r == 1)
        def _():
            pltpu.make_async_copy(ow, ow, weight_sems.at[2]).wait()
            ow_copy.start()

        rows = pl.ds(pl.multiple_of(r * ROWS, ROWS), ROWS)
        scale = HEAD_DIM**-0.5
        scaled_cos, scaled_sin = cosine[rows, :] * scale, sine[rows, :] * scale
        for c in range(wq.shape[1] // COLS):
            part = jnp.dot(
                tok[rows, :], wq[:, c * COLS : (c + 1) * COLS], preferred_element_type=f32
            )
            for k in range(COLS // LANES):
                turned = turn(part[:, k * LANES : (k + 1) * LANES], scaled_cos, scaled_sin)
                away = pltpu.roll(turned, HEAD_DIM, 1)
                for j in range(2):
                    head = 2 * (c * (COLS // LANES) + k) + j
                    group, m = head // slices, head % slices
                    lanes = slice(group * HEAD_DIM, (group + 1) * HEAD_DIM)
                    at = m * LANES + group * HEAD_DIM
                    queries[rows, at : at + HEAD_DIM] = (
                        turned if group == j else away
                    )[:, lanes].astype(bf16)

    key_count = devices * KEY_BLOCK + QUERY_BLOCK

    blocks_in = ROWS // QUERY_BLOCK

    def group_of(b):
        return b // blocks_in + jnp.where(b == last, 1, 0)

    def wait_mix(first, count):
        rows = pl.ds(pl.multiple_of(first * QUERY_BLOCK, QUERY_BLOCK), count * QUERY_BLOCK)
        landed = mix_other.at[rows]
        pltpu.make_async_copy(landed, landed, mix_recv.at[group_of(first)]).wait()

    def mix_copy(b):
        rows = pl.ds(pl.multiple_of(b * QUERY_BLOCK, QUERY_BLOCK), QUERY_BLOCK)
        return pltpu.make_async_remote_copy(
            src_ref=mix.at[rows],
            dst_ref=mix_other.at[rows] if b is not last else mix_end,
            send_sem=mix_send.at[0],
            recv_sem=mix_recv.at[group_of(b)],
            device_id={"tp": other},
            device_id_type=MESH,
        )

    low_mask = jnp.where(low_lanes((key_count, LANES)), 1.0, 0.0).astype(bf16)
    high_mask = jnp.where(low_lanes((key_count, LANES)), 0.0, 1.0).astype(bf16)

    def wait_kv(b, lanes, sem):
        for n in range(1, devices):

            @pl.when(me == n)
            def _():
                landed = pool.at[pl.ds(b * devices, n), :, lanes]
                pltpu.make_async_copy(landed, landed, kv_recv.at[sem]).wait()

    def block_of(b, lanes):
        far = pool[pl.ds(b * devices, devices), :, lanes].reshape(devices * KEY_BLOCK, LANES)
        near = kv[pl.ds(b * per_q, per_q), :, lanes].reshape(QUERY_BLOCK, LANES)
        return jnp.concatenate([far, near], axis=0)

    sections = [slice(m * QUERY_BLOCK, (m + 1) * QUERY_BLOCK) for m in range(slices)]

    def attend_keys(b):
        row = me * qblocks + b
        rows = pl.ds(pl.multiple_of(b * QUERY_BLOCK, QUERY_BLOCK), QUERY_BLOCK)
        keys = block_of(b, slice(0, LANES))
        owner = lax.broadcasted_iota(jnp.int32, (1, devices * KEY_BLOCK), 1) // KEY_BLOCK
        bias = jnp.full((1, devices * KEY_BLOCK), hidden, f32)
        for s in range(chosen):
            bias = jnp.where(owner == owner_ref[s, row], 0.0, bias)
        bias = jnp.broadcast_to(bias, (QUERY_BLOCK, devices * KEY_BLOCK)).astype(bf16)
        bias = jnp.concatenate([bias, causal[...]], axis=1)
        turned = keys.T
        blank = jnp.zeros((HEAD_DIM, key_count), bf16)
        wide_keys = jnp.concatenate(
            [
                jnp.concatenate([turned[:HEAD_DIM], blank, bias], axis=0),
                jnp.concatenate([blank, turned[HEAD_DIM:], bias], axis=0),
            ],
            axis=1,
        )
        keys_now[...] = wide_keys
        for m, section in enumerate(sections):
            q = jnp.concatenate([queries[rows, m * LANES : (m + 1) * LANES], eye[...]], axis=1)
            scores[section, :] = jnp.dot(q, keys_now[...], preferred_element_type=f32)
        for section in sections:
            for side in range(2):
                cols = slice(side * key_count, (side + 1) * key_count)
                s = scores[section, cols]
                weights[section, cols] = jnp.exp(s - jnp.max(s, axis=1, keepdims=True)).astype(bf16)

    def attend_values(b):
        rows = pl.ds(pl.multiple_of(b * QUERY_BLOCK, QUERY_BLOCK), QUERY_BLOCK)
        values = block_of(b, slice(LANES, 2 * LANES))
        values_now[...] = jnp.concatenate(
            [
                jnp.concatenate([values * low_mask, low_mask], axis=1),
                jnp.concatenate([values * high_mask, high_mask], axis=1),
            ],
            axis=0,
        )
        for m, section in enumerate(sections):
            mixed = jnp.dot(weights[section, :], values_now[...], preferred_element_type=f32)
            mix[rows, m * LANES : (m + 1) * LANES] = (mixed[:, :LANES] / mixed[:, LANES:]).astype(
                bf16
            )
        mix_copy(b).start()

    def ss_copy(b):
        return pltpu.make_async_remote_copy(
            src_ref=ss.at[b],
            dst_ref=ss_other.at[b],
            send_sem=ss_send.at[0],
            recv_sem=ss_recv.at[group_of(b)],
            device_id={"tp": other},
            device_id_type=MESH,
        )

    def project_mine(first):
        rows = pl.ds(pl.multiple_of(first * QUERY_BLOCK, QUERY_BLOCK), QUERY_BLOCK)
        for c in range(half // COLS):
            early[:, c * COLS : (c + 1) * COLS] = part_of(mix, ow, rows, half, core, c)

    def project(first, count, ready=False):
        wait_mix(first, count)
        size = count * QUERY_BLOCK
        rows = pl.ds(pl.multiple_of(first * QUERY_BLOCK, QUERY_BLOCK), size)
        total = jnp.zeros((size, LANES), f32)
        for c in range(half // COLS):
            at = slice(c * COLS, (c + 1) * COLS)
            mine = early[:, at] if ready else part_of(mix, ow, rows, half, core, c)
            theirs = part_of(mix_other, ow_other, rows, half, core, c)
            added = mine.astype(f32) + theirs.astype(f32)
            proj[rows, at] = added
            total = squares(total, added)
        for j in range(count):
            ss[first + j] = total[j * QUERY_BLOCK : (j + 1) * QUERY_BLOCK]
            ss_copy(first + j).start()

    def normed(rows, total):
        scale = row_scale(total, half)
        for c in range(half // LANES):
            at = slice(c * LANES, (c + 1) * LANES)
            out[rows, at] = (proj[rows, at] * scale * gain[:, at]).astype(bf16)

    def norm(first, count):
        landed = ss_other.at[pl.ds(first, count)]
        pltpu.make_async_copy(landed, landed, ss_recv.at[group_of(first)]).wait()

        @pl.loop(0, count)
        def _(j):
            b = first + j
            rows = pl.ds(pl.multiple_of(b * QUERY_BLOCK, QUERY_BLOCK), QUERY_BLOCK)
            normed(rows, ss[b] + ss_other[b])

    @pl.loop(0, last)
    def _(b):
        wait_kv(b, all_lanes, b)
        attend_keys(b)
        attend_values(b)

        @pl.when(b == 1)
        def _():
            ow_copy.wait_recv()

        @pl.when(jnp.logical_and(paced, jnp.logical_and(b > 0, b < last - 2)))
        def _():
            send_block(b + 1, False)

        @pl.when(b % blocks_in == blocks_in - 1)
        def _():
            project(b + 1 - blocks_in, blocks_in)

        @pl.when(jnp.logical_and(paced, b == last - 2))
        def _():
            send_block(last - 1, False)

        @pl.when(jnp.logical_and(b > 0, b % blocks_in == 0))
        def _():
            norm(b - blocks_in, blocks_in)

    @pl.when(paced)
    def _():
        send_block(last, True)

    project_mine(last - 1)
    gain_end[...] = gain[...]
    wait_kv(last, key_lanes, last)
    attend_keys(last)
    wait_kv(last, value_lanes, qblocks)
    attend_values(last)
    project(last - 1, 1, ready=True)
    final = slice(last * QUERY_BLOCK, qblocks * QUERY_BLOCK)
    for n, side in enumerate((other, core)):
        for c in range(half // COLS):
            at = n * half + c * COLS
            partial[:, at : at + COLS] = part_of(mix, ow, final, half, side, c)

    @pl.loop(0, devices)
    def _(dst):
        @pl.when(dst > me)
        def _():
            sent = send.at[pl.ds(dst * qblocks, qblocks)]
            pltpu.make_async_copy(sent, sent, kv_send.at[dst]).wait()

    ow_copy.wait_send()
    pltpu.make_async_copy(ss.at[pl.ds(0, last)], ss.at[pl.ds(0, last)], ss_send.at[0]).wait()
    pltpu.make_async_copy(mix_end, mix_end, mix_recv.at[group_of(last)]).wait()
    pltpu.make_async_copy(mix, mix, mix_send.at[0]).wait()
    norm(last - 1, 1)


def finish_kernel(held, mix_end, ow_other, partial, gain, out, proj, end, sems):
    core = lax.axis_index("tp")
    half = gain.shape[1]
    early = held.shape[0] - QUERY_BLOCK
    rows = pl.ds(0, early)
    first = pltpu.make_async_copy(held.at[rows], out.at[rows], sems.at[0])
    first.start()
    every = slice(0, QUERY_BLOCK)
    total = jnp.zeros((QUERY_BLOCK, LANES), jnp.float32)
    for n, side in enumerate((1 - core, core)):
        for c in range(half // COLS):
            at = n * half + c * COLS
            theirs = part_of(mix_end, ow_other, every, half, side, c)
            mine = partial[:, at : at + COLS]
            added = mine.astype(jnp.float32) + theirs.astype(jnp.float32)
            if side is core:
                proj[:, c * COLS : (c + 1) * COLS] = added
            total = squares(total, added)
    scale = row_scale(total, half)
    for c in range(half // LANES):
        at = slice(c * LANES, (c + 1) * LANES)
        end[:, at] = (proj[:, at] * scale * gain[:, at]).astype(jnp.bfloat16)
    final = pltpu.make_async_copy(end, out.at[pl.ds(early, QUERY_BLOCK)], sems.at[1])
    final.start()
    first.wait()
    final.wait()


def trig_table(devices, blocks):
    half_dim = HEAD_DIM // 2
    lane = np.arange(LANES)
    frequency = (rope_base ** (-(lane % half_dim) / half_dim)).astype(np.float32)
    sign = np.where(lane % HEAD_DIM < half_dim, -1.0, 1.0)
    near = np.arange(QUERY_BLOCK)[:, None] * frequency.astype(np.float64)
    far = (np.arange(blocks)[:, None] * np.float32(QUERY_BLOCK) * frequency).astype(np.float64)
    near = np.concatenate([np.cos(near), sign * np.sin(near)], axis=0)
    far = np.stack([np.cos(far), sign * np.sin(far)]).reshape(2, devices, -1, LANES)
    far = far.transpose(1, 0, 2, 3).reshape(devices, -1, LANES)
    return near.astype(np.float32), far.astype(np.float32)


def body(
    tokens, query_weight, key_weight, value_weight, out_weight, norm_gain, chosen_owner, chosen_part
):
    row_data = tokens[0]
    count = row_data.shape[0]
    devices = lax.axis_size("kv")
    qblocks = count // QUERY_BLOCK
    heads_width = query_weight.shape[1]
    half = norm_gain.shape[0]
    hbm = pl.BlockSpec(memory_space=pl.ANY)
    vmem = pl.BlockSpec(memory_space=pltpu.VMEM)
    bf16, f32 = jnp.bfloat16, jnp.float32
    slots = chosen_owner.shape[1:][::-1]
    key_count = devices * KEY_BLOCK + QUERY_BLOCK
    near_trig, far_trig = trig_table(devices, devices * qblocks)
    operands = [
        chosen_owner[0].T, chosen_part[0].T, row_data, query_weight, key_weight, value_weight,
        out_weight, norm_gain[None], jnp.asarray(near_trig), jnp.asarray(far_trig),
    ]
    operands = [pltpu.with_memory_space_constraint(x, pltpu.HBM) for x in operands]
    result = pl.pallas_call(
        functools.partial(kernel, devices),
        out_shape=[
            pltpu.VMEM((count, half), bf16),
            pltpu.VMEM((QUERY_BLOCK, heads_width), bf16),
            pltpu.VMEM(out_weight.shape, bf16),
            pltpu.VMEM((QUERY_BLOCK, 2 * half), bf16),
            pltpu.VMEM((1, half), f32),
        ],
        in_specs=[hbm] * len(operands),
        out_specs=[vmem] * 5,
        scratch_shapes=[
            pltpu.SMEM(slots, jnp.int32),
            pltpu.SMEM(slots, jnp.int32),
            pltpu.VMEM((1, half), f32),
            pltpu.VMEM(near_trig.shape, f32),
            pltpu.VMEM(far_trig.shape[1:], f32),
            pltpu.SemaphoreType.DMA((5,)),
            pltpu.VMEM((count, LANES), f32),
            pltpu.VMEM((count, LANES), f32),
            pltpu.VMEM((QUERY_BLOCK, QUERY_BLOCK), bf16),
            pltpu.VMEM((QUERY_BLOCK, QUERY_BLOCK), bf16),
            pltpu.VMEM(row_data.shape, bf16),
            pltpu.VMEM(query_weight.shape, bf16),
            pltpu.VMEM((key_weight.shape[0], 2 * key_weight.shape[1]), bf16),
            pltpu.VMEM(out_weight.shape, bf16),
            pltpu.SemaphoreType.DMA((2,)),
            pltpu.SemaphoreType.DMA((3,)),
            pltpu.VMEM((count // KEY_BLOCK, KEY_BLOCK, 2 * LANES), bf16),
            pltpu.VMEM((devices * qblocks, KEY_BLOCK, 2 * LANES), bf16),
            pltpu.VMEM((devices * qblocks, KEY_BLOCK, 2 * LANES), bf16),
            pltpu.VMEM((count, heads_width), bf16),
            pltpu.VMEM((LANES + QUERY_BLOCK, 2 * key_count), bf16),
            pltpu.VMEM((2 * key_count, 2 * LANES), bf16),
            pltpu.VMEM((heads_width // LANES * QUERY_BLOCK, 2 * key_count), f32),
            pltpu.VMEM((heads_width // LANES * QUERY_BLOCK, 2 * key_count), bf16),
            pltpu.VMEM((count, heads_width), bf16),
            pltpu.VMEM((count, heads_width), bf16),
            pltpu.VMEM((QUERY_BLOCK, half), bf16),
            pltpu.VMEM((count, half), f32),
            pltpu.VMEM((qblocks, QUERY_BLOCK, LANES), f32),
            pltpu.VMEM((qblocks, QUERY_BLOCK, LANES), f32),
            pltpu.SemaphoreType.DMA((devices,)),
            pltpu.SemaphoreType.DMA((qblocks + 1,)),
            pltpu.SemaphoreType.DMA((2,)),
            pltpu.SemaphoreType.DMA((1,)),
            pltpu.SemaphoreType.DMA((count // ROWS + 1,)),
            pltpu.SemaphoreType.DMA((1,)),
            pltpu.SemaphoreType.DMA((count // ROWS,)),
        ],
        compiler_params=pltpu.CompilerParams(
            collective_id=0, has_side_effects=True, vmem_limit_bytes=48 * 1024 * 1024
        ),
    )(*operands)
    result = [pltpu.with_memory_space_constraint(x, pltpu.VMEM) for x in result]
    return pl.pallas_call(
        finish_kernel,
        out_shape=jax.ShapeDtypeStruct((count, half), bf16),
        in_specs=[vmem] * len(result),
        out_specs=hbm,
        scratch_shapes=[
            pltpu.VMEM((QUERY_BLOCK, half), f32),
            pltpu.VMEM((QUERY_BLOCK, half), bf16),
            pltpu.SemaphoreType.DMA((2,)),
        ],
        compiler_params=pltpu.CompilerParams(vmem_limit_bytes=8 * 1024 * 1024),
    )(*result)[None]


def solution(mesh):
    placed = (
        P("dp", "kv", None),
        P(None, "tp"),
        P(None, "tp"),
        P(None, "tp"),
        P("tp", None),
        P("tp"),
        P("dp", None, None),
        P("dp", None, None),
    )
    return jax.shard_map(
        body, mesh=mesh, in_specs=placed, out_specs=P("dp", "kv", "tp"), check_vma=False
    )
```

```python
import functools

import jax
import jax.numpy as jnp
import numpy as np
from jax import lax
from jax.experimental import pallas as pl
from jax.experimental.pallas import tpu as pltpu
from jax.sharding import PartitionSpec as P

HEAD_DIM = 64
QUERY_BLOCK = 128
KEY_BLOCK = 64
LANES = 128
ROWS = 256
COLS = 256

rope_base = 10000.0
norm_eps = 1e-06
hidden = -1e38
MESH = pl.DeviceIdType.MESH


def low_lanes(shape):
    return lax.broadcasted_iota(jnp.int32, shape, 1) < HEAD_DIM


def turn(u, cosine, sine):
    lane = lax.broadcasted_iota(jnp.int32, u.shape, 1)
    half = HEAD_DIM // 2
    swapped = jnp.where(
        lane % HEAD_DIM < half, pltpu.roll(u, LANES - half, 1), pltpu.roll(u, half, 1)
    )
    return u * cosine + swapped * sine


def part_of(left, right, rows, half, side, c):
    cols = pl.ds(pl.multiple_of(side * half + c * COLS, COLS), COLS)
    return jnp.dot(
        left[rows, :], right[:, cols], preferred_element_type=jnp.float32
    ).astype(jnp.bfloat16)


def squares(total, added):
    for k in range(COLS // LANES):
        piece = added[:, k * LANES : (k + 1) * LANES]
        total = total + piece * piece
    return total


def row_scale(total, half):
    return lax.rsqrt(jnp.sum(total, axis=1, keepdims=True) / (2 * half) + norm_eps)


def kernel(
    devices, owner_hbm, part_hbm, tok_hbm, wq_hbm, wk_hbm, wv_hbm, ow_hbm, gain_hbm, near_hbm, far_hbm, out, mix_end, ow_other, partial, gain_end,
    owner_ref, part_ref, gain, near_trig, far_trig, small_sems, cosine, sine, eye, causal,
    tok, wq, wkv, ow, tok_sems, weight_sems,
    kv, send, pool, queries, keys_now, values_now, scores, weights, mix, mix_other, early, proj, ss, ss_other,
    kv_send, kv_recv, ow_sems, mix_send, mix_recv, ss_send, ss_recv,
):
    me = lax.axis_index("kv")
    core = lax.axis_index("tp")
    other = 1 - core
    tokens = tok.shape[0]
    qblocks = tokens // QUERY_BLOCK
    chosen = owner_ref.shape[0]
    half = gain.shape[1]
    row_steps = tokens // ROWS
    per_q = QUERY_BLOCK // KEY_BLOCK
    key_width = wk_hbm.shape[1]
    slices = wq.shape[1] // LANES
    heads = wq.shape[1] // HEAD_DIM
    bf16, f32 = jnp.bfloat16, jnp.float32

    pieces = ((0, ROWS), (ROWS, tokens - ROWS))

    def tok_copy(r):
        rows = pl.ds(*pieces[r])
        return pltpu.make_async_copy(tok_hbm.at[rows], tok.at[rows], tok_sems.at[r])

    wk_copy = pltpu.make_async_copy(wk_hbm, wkv.at[:, pl.ds(0, key_width)], weight_sems.at[0])
    wv_copy = pltpu.make_async_copy(
        wv_hbm, wkv.at[:, pl.ds(key_width, key_width)], weight_sems.at[0]
    )
    wq_copy = pltpu.make_async_copy(wq_hbm, wq, weight_sems.at[1])
    ow_loads = []
    for m in range(slices):
        for g in range(2):
            ow_loads.append(
                pltpu.make_async_copy(
                    ow_hbm.at[pl.ds((g * slices + m) * HEAD_DIM, HEAD_DIM)],
                    ow.at[pl.ds((2 * m + g) * HEAD_DIM, HEAD_DIM)],
                    weight_sems.at[2],
                )
            )
    small = [
        pltpu.make_async_copy(near_hbm, near_trig, small_sems.at[0]),
        pltpu.make_async_copy(far_hbm.at[me], far_trig, small_sems.at[4]),
        pltpu.make_async_copy(owner_hbm, owner_ref, small_sems.at[1]),
        pltpu.make_async_copy(part_hbm, part_ref, small_sems.at[2]),
        pltpu.make_async_copy(gain_hbm, gain, small_sems.at[3]),
    ]
    small[0].start()
    small[1].start()
    wk_copy.start()
    wv_copy.start()
    tok_copy(0).start()
    tok_copy(1).start(priority=1)
    for copy in small[2:]:
        copy.start(priority=1)

    barrier = pltpu.get_barrier_semaphore()

    @pl.loop(0, devices)
    def _(j):
        @pl.when(j != me)
        def _():
            pl.semaphore_signal(barrier, inc=1, device_id={"kv": j}, device_id_type=MESH)

    pl.semaphore_signal(barrier, inc=1, device_id={"tp": other}, device_id_type=MESH)

    square = (QUERY_BLOCK, QUERY_BLOCK)
    first = lax.broadcasted_iota(jnp.int32, square, 0)
    second = lax.broadcasted_iota(jnp.int32, square, 1)
    eye[...] = jnp.where(first == second, 1.0, 0.0).astype(bf16)
    causal[...] = jnp.where(first >= second, 0.0, hidden).astype(bf16)

    small[0].wait()
    small[1].wait()
    near_cos = near_trig[0:QUERY_BLOCK, :]
    near_sin = near_trig[QUERY_BLOCK : 2 * QUERY_BLOCK, :]

    @pl.loop(0, qblocks)
    def _(b):
        rows = pl.ds(pl.multiple_of(b * QUERY_BLOCK, QUERY_BLOCK), QUERY_BLOCK)
        far_cos = far_trig[pl.ds(b, 1), :]
        far_sin = far_trig[pl.ds(b + qblocks, 1), :]
        cosine[rows, :] = far_cos * near_cos - far_sin * near_sin
        sine[rows, :] = far_sin * near_cos + far_cos * near_sin

    pltpu.make_async_copy(wkv, wkv, weight_sems.at[0]).wait()

    once = jnp.where(core >= 0, 1, 0)
    for r, (start, size) in enumerate(pieces):

        @pl.loop(0, once)
        def _(_):
            tok_copy(r).wait()
            if r == 0:
                wq_copy.start(priority=1)
                for copy in ow_loads:
                    copy.start(priority=1)
            rows = pl.ds(start, size)
            both = jnp.dot(tok[rows, :], wkv[...], preferred_element_type=f32)
            keys = turn(both[:, :LANES], cosine[rows, :], sine[rows, :])
            joined = jnp.concatenate([keys, both[:, LANES:]], axis=1).astype(bf16)
            blocks = size // KEY_BLOCK
            kv[pl.ds(start // KEY_BLOCK, blocks)] = joined.reshape(blocks, KEY_BLOCK, 2 * LANES)

    for copy in small[2:]:
        copy.wait()
    pl.semaphore_wait(barrier, devices)

    def place(src, row, s):
        return owner_ref[s, row] == src, part_ref[s, row]

    def wanted(dst, q):
        found = [place(me, dst * qblocks + q, s) for s in range(chosen)]
        return sum(jnp.where(here, at, 0) for here, at in found)

    def kv_copy(dst, q, lanes, sem):
        return pltpu.make_async_remote_copy(
            src_ref=send.at[pl.ds(dst * qblocks + q, 1), :, lanes],
            dst_ref=pool.at[pl.ds(q * devices + me, 1), :, lanes],
            send_sem=kv_send.at[dst],
            recv_sem=kv_recv.at[sem],
            device_id={"kv": dst},
            device_id_type=MESH,
        )

    last = qblocks - 1
    all_lanes, key_lanes, value_lanes = (
        pl.ds(0, 2 * LANES), pl.ds(0, LANES), pl.ds(LANES, LANES)
    )

    def send_block(q, split):
        @pl.loop(0, devices - 1)
        def _(step):
            dst = devices - 1 - step

            @pl.when(dst > me)
            def _():
                send[pl.ds(dst * qblocks + q, 1)] = kv[pl.ds(wanted(dst, q), 1)]
                kv_copy(dst, q, key_lanes if split else all_lanes, q).start()

        if split:

            @pl.loop(1, devices)
            def _(dst):
                @pl.when(dst > me)
                def _():
                    kv_copy(dst, q, value_lanes, qblocks).start()

    paced = me + 3 < devices

    @pl.loop(0, jnp.where(paced, 1, last))
    def _(q):
        send_block(q, False)

    @pl.when(jnp.logical_not(paced))
    def _():
        send_block(last, True)

    @pl.loop(0, qblocks)
    def _(q):
        pool[pl.ds(q * devices + me, 1)] = kv[pl.ds(wanted(me, q), 1)]

        @pl.loop(0, devices)
        def _(src):
            @pl.when(src > me)
            def _():
                pool[pl.ds(q * devices + src, 1)] = jnp.zeros((1, KEY_BLOCK, 2 * LANES), bf16)

    ow_copy = pltpu.make_async_remote_copy(
        src_ref=ow,
        dst_ref=ow_other,
        send_sem=ow_sems.at[0],
        recv_sem=ow_sems.at[1],
        device_id={"tp": other},
        device_id_type=MESH,
    )
    wq_copy.wait()

    @pl.loop(0, row_steps)
    def _(r):
        @pl.when(jnp.logical_and(paced, r == row_steps - 1))
        def _():
            send_block(1, False)

        @pl.when(r == 1)
        def _():
            pltpu.make_async_copy(ow, ow, weight_sems.at[2]).wait()
            ow_copy.start()

        rows = pl.ds(pl.multiple_of(r * ROWS, ROWS), ROWS)
        scale = HEAD_DIM**-0.5
        scaled_cos, scaled_sin = cosine[rows, :] * scale, sine[rows, :] * scale
        for c in range(wq.shape[1] // COLS):
            part = jnp.dot(
                tok[rows, :], wq[:, c * COLS : (c + 1) * COLS], preferred_element_type=f32
            )
            for k in range(COLS // LANES):
                turned = turn(part[:, k * LANES : (k + 1) * LANES], scaled_cos, scaled_sin)
                away = pltpu.roll(turned, HEAD_DIM, 1)
                for j in range(2):
                    head = 2 * (c * (COLS // LANES) + k) + j
                    group, m = head // slices, head % slices
                    lanes = slice(group * HEAD_DIM, (group + 1) * HEAD_DIM)
                    at = m * LANES + group * HEAD_DIM
                    queries[rows, at : at + HEAD_DIM] = (
                        turned if group == j else away
                    )[:, lanes].astype(bf16)

    key_count = devices * KEY_BLOCK + QUERY_BLOCK

    blocks_in = ROWS // QUERY_BLOCK

    def group_of(b):
        return b // blocks_in + jnp.where(b == last, 1, 0)

    def wait_mix(first, count):
        rows = pl.ds(pl.multiple_of(first * QUERY_BLOCK, QUERY_BLOCK), count * QUERY_BLOCK)
        landed = mix_other.at[rows]
        pltpu.make_async_copy(landed, landed, mix_recv.at[group_of(first)]).wait()

    def mix_copy(b):
        rows = pl.ds(pl.multiple_of(b * QUERY_BLOCK, QUERY_BLOCK), QUERY_BLOCK)
        return pltpu.make_async_remote_copy(
            src_ref=mix.at[rows],
            dst_ref=mix_other.at[rows] if b is not last else mix_end,
            send_sem=mix_send.at[0],
            recv_sem=mix_recv.at[group_of(b)],
            device_id={"tp": other},
            device_id_type=MESH,
        )

    low_mask = jnp.where(low_lanes((key_count, LANES)), 1.0, 0.0).astype(bf16)
    high_mask = jnp.where(low_lanes((key_count, LANES)), 0.0, 1.0).astype(bf16)

    def wait_kv(b, lanes, sem):
        for n in range(1, devices):

            @pl.when(me == n)
            def _():
                landed = pool.at[pl.ds(b * devices, n), :, lanes]
                pltpu.make_async_copy(landed, landed, kv_recv.at[sem]).wait()

    def block_of(b, lanes):
        far = pool[pl.ds(b * devices, devices), :, lanes].reshape(devices * KEY_BLOCK, LANES)
        near = kv[pl.ds(b * per_q, per_q), :, lanes].reshape(QUERY_BLOCK, LANES)
        return jnp.concatenate([far, near], axis=0)

    sections = [slice(m * QUERY_BLOCK, (m + 1) * QUERY_BLOCK) for m in range(slices)]

    def attend_keys(b):
        row = me * qblocks + b
        rows = pl.ds(pl.multiple_of(b * QUERY_BLOCK, QUERY_BLOCK), QUERY_BLOCK)
        keys = block_of(b, slice(0, LANES))
        owner = lax.broadcasted_iota(jnp.int32, (1, devices * KEY_BLOCK), 1) // KEY_BLOCK
        bias = jnp.full((1, devices * KEY_BLOCK), hidden, f32)
        for s in range(chosen):
            bias = jnp.where(owner == owner_ref[s, row], 0.0, bias)
        bias = jnp.broadcast_to(bias, (QUERY_BLOCK, devices * KEY_BLOCK)).astype(bf16)
        bias = jnp.concatenate([bias, causal[...]], axis=1)
        turned = keys.T
        blank = jnp.zeros((HEAD_DIM, key_count), bf16)
        wide_keys = jnp.concatenate(
            [
                jnp.concatenate([turned[:HEAD_DIM], blank, bias], axis=0),
                jnp.concatenate([blank, turned[HEAD_DIM:], bias], axis=0),
            ],
            axis=1,
        )
        keys_now[...] = wide_keys
        for m, section in enumerate(sections):
            q = jnp.concatenate([queries[rows, m * LANES : (m + 1) * LANES], eye[...]], axis=1)
            scores[section, :] = jnp.dot(q, keys_now[...], preferred_element_type=f32)
        for section in sections:
            for side in range(2):
                cols = slice(side * key_count, (side + 1) * key_count)
                s = scores[section, cols]
                weights[section, cols] = jnp.exp(s - jnp.max(s, axis=1, keepdims=True)).astype(bf16)

    def attend_values(b):
        rows = pl.ds(pl.multiple_of(b * QUERY_BLOCK, QUERY_BLOCK), QUERY_BLOCK)
        values = block_of(b, slice(LANES, 2 * LANES))
        values_now[...] = jnp.concatenate(
            [
                jnp.concatenate([values * low_mask, low_mask], axis=1),
                jnp.concatenate([values * high_mask, high_mask], axis=1),
            ],
            axis=0,
        )
        for m, section in enumerate(sections):
            mixed = jnp.dot(weights[section, :], values_now[...], preferred_element_type=f32)
            mix[rows, m * LANES : (m + 1) * LANES] = (mixed[:, :LANES] / mixed[:, LANES:]).astype(
                bf16
            )
        mix_copy(b).start()

    def ss_copy(b):
        return pltpu.make_async_remote_copy(
            src_ref=ss.at[b],
            dst_ref=ss_other.at[b],
            send_sem=ss_send.at[0],
            recv_sem=ss_recv.at[group_of(b)],
            device_id={"tp": other},
            device_id_type=MESH,
        )

    def project_mine(first, held):
        rows = pl.ds(first * QUERY_BLOCK, QUERY_BLOCK)
        for n, side in enumerate((other, core)):
            for c in range(half // COLS):
                at = n * half + c * COLS
                held[:, at : at + COLS] = part_of(mix, ow, rows, half, side, c)

    def project_whole(first):
        wait_mix(first, 1)
        rows = pl.ds(first * QUERY_BLOCK, QUERY_BLOCK)
        total = jnp.zeros((QUERY_BLOCK, LANES), f32)
        for n, side in enumerate((other, core)):
            for c in range(half // COLS):
                at = n * half + c * COLS
                theirs = part_of(mix_other, ow_other, rows, half, side, c)
                added = early[:, at : at + COLS].astype(f32) + theirs.astype(f32)
                if side is core:
                    proj[rows, c * COLS : (c + 1) * COLS] = added
                total = squares(total, added)
        normed(rows, total)

    def project(first, count):
        wait_mix(first, count)
        size = count * QUERY_BLOCK
        rows = pl.ds(pl.multiple_of(first * QUERY_BLOCK, QUERY_BLOCK), size)
        total = jnp.zeros((size, LANES), f32)
        for c in range(half // COLS):
            at = slice(c * COLS, (c + 1) * COLS)
            mine = part_of(mix, ow, rows, half, core, c)
            theirs = part_of(mix_other, ow_other, rows, half, core, c)
            added = mine.astype(f32) + theirs.astype(f32)
            proj[rows, at] = added
            total = squares(total, added)
        for j in range(count):
            ss[first + j] = total[j * QUERY_BLOCK : (j + 1) * QUERY_BLOCK]
            ss_copy(first + j).start()

    def normed(rows, total):
        scale = row_scale(total, half)
        for c in range(half // LANES):
            at = slice(c * LANES, (c + 1) * LANES)
            out[rows, at] = (proj[rows, at] * scale * gain[:, at]).astype(bf16)

    def norm(first, count):
        landed = ss_other.at[pl.ds(first, count)]
        pltpu.make_async_copy(landed, landed, ss_recv.at[group_of(first)]).wait()

        size = count * QUERY_BLOCK
        rows = pl.ds(pl.multiple_of(first * QUERY_BLOCK, QUERY_BLOCK), size)
        blocks = pl.ds(first, count)
        normed(rows, (ss[blocks] + ss_other[blocks]).reshape(size, LANES))

    @pl.loop(0, last)
    def _(b):
        wait_kv(b, all_lanes, b)
        attend_keys(b)
        attend_values(b)

        @pl.when(b == 1)
        def _():
            ow_copy.wait_recv()

        @pl.when(jnp.logical_and(paced, jnp.logical_and(b > 0, b < last - 2)))
        def _():
            send_block(b + 1, False)

        @pl.when(b % blocks_in == blocks_in - 1)
        def _():
            project(b + 1 - blocks_in, blocks_in)

        @pl.when(jnp.logical_and(paced, b == last - 2))
        def _():
            send_block(last - 1, False)

        @pl.when(jnp.logical_and(b > 0, b % blocks_in == 0))
        def _():
            norm(b - blocks_in, blocks_in)

    @pl.when(paced)
    def _():
        send_block(last, True)

    project_mine(last - 1, early)
    gain_end[...] = gain[...]
    wait_kv(last, key_lanes, last)
    attend_keys(last)
    wait_kv(last, value_lanes, qblocks)
    attend_values(last)
    project_mine(last, partial)
    project_whole(last - 1)

    @pl.loop(0, devices)
    def _(dst):
        @pl.when(dst > me)
        def _():
            sent = send.at[pl.ds(dst * qblocks, qblocks)]
            pltpu.make_async_copy(sent, sent, kv_send.at[dst]).wait()

    ow_copy.wait_send()
    shared = ss.at[pl.ds(0, last - 1)]
    pltpu.make_async_copy(shared, shared, ss_send.at[0]).wait()
    pltpu.make_async_copy(mix_end, mix_end, mix_recv.at[group_of(last)]).wait()
    pltpu.make_async_copy(mix, mix, mix_send.at[0]).wait()


def finish_kernel(held, mix_end, ow_other, partial, gain, out, proj, end, sems):
    core = lax.axis_index("tp")
    half = gain.shape[1]
    early = held.shape[0] - QUERY_BLOCK
    rows = pl.ds(0, early)
    first = pltpu.make_async_copy(held.at[rows], out.at[rows], sems.at[0])
    first.start()
    every = slice(0, QUERY_BLOCK)
    total = jnp.zeros((QUERY_BLOCK, LANES), jnp.float32)
    for n, side in enumerate((1 - core, core)):
        for c in range(half // COLS):
            at = n * half + c * COLS
            theirs = part_of(mix_end, ow_other, every, half, side, c)
            mine = partial[:, at : at + COLS]
            added = mine.astype(jnp.float32) + theirs.astype(jnp.float32)
            if side is core:
                proj[:, c * COLS : (c + 1) * COLS] = added
            total = squares(total, added)
    scale = row_scale(total, half)
    for c in range(half // LANES):
        at = slice(c * LANES, (c + 1) * LANES)
        end[:, at] = (proj[:, at] * scale * gain[:, at]).astype(jnp.bfloat16)
    final = pltpu.make_async_copy(end, out.at[pl.ds(early, QUERY_BLOCK)], sems.at[1])
    final.start()
    first.wait()
    final.wait()


def trig_table(devices, blocks):
    half_dim = HEAD_DIM // 2
    lane = np.arange(LANES)
    frequency = (rope_base ** (-(lane % half_dim) / half_dim)).astype(np.float32)
    sign = np.where(lane % HEAD_DIM < half_dim, -1.0, 1.0)
    near = np.arange(QUERY_BLOCK)[:, None] * frequency.astype(np.float64)
    far = (np.arange(blocks)[:, None] * np.float32(QUERY_BLOCK) * frequency).astype(np.float64)
    near = np.concatenate([np.cos(near), sign * np.sin(near)], axis=0)
    far = np.stack([np.cos(far), sign * np.sin(far)]).reshape(2, devices, -1, LANES)
    far = far.transpose(1, 0, 2, 3).reshape(devices, -1, LANES)
    return near.astype(np.float32), far.astype(np.float32)


def body(
    tokens, query_weight, key_weight, value_weight, out_weight, norm_gain, chosen_owner, chosen_part
):
    row_data = tokens[0]
    count = row_data.shape[0]
    devices = lax.axis_size("kv")
    qblocks = count // QUERY_BLOCK
    heads_width = query_weight.shape[1]
    half = norm_gain.shape[0]
    hbm = pl.BlockSpec(memory_space=pl.ANY)
    vmem = pl.BlockSpec(memory_space=pltpu.VMEM)
    bf16, f32 = jnp.bfloat16, jnp.float32
    slots = chosen_owner.shape[1:][::-1]
    key_count = devices * KEY_BLOCK + QUERY_BLOCK
    near_trig, far_trig = trig_table(devices, devices * qblocks)
    operands = [
        chosen_owner[0].T, chosen_part[0].T, row_data, query_weight, key_weight, value_weight,
        out_weight, norm_gain[None], jnp.asarray(near_trig), jnp.asarray(far_trig),
    ]
    operands = [pltpu.with_memory_space_constraint(x, pltpu.HBM) for x in operands]
    result = pl.pallas_call(
        functools.partial(kernel, devices),
        out_shape=[
            pltpu.VMEM((count, half), bf16),
            pltpu.VMEM((QUERY_BLOCK, heads_width), bf16),
            pltpu.VMEM(out_weight.shape, bf16),
            pltpu.VMEM((QUERY_BLOCK, 2 * half), bf16),
            pltpu.VMEM((1, half), f32),
        ],
        in_specs=[hbm] * len(operands),
        out_specs=[vmem] * 5,
        scratch_shapes=[
            pltpu.SMEM(slots, jnp.int32),
            pltpu.SMEM(slots, jnp.int32),
            pltpu.VMEM((1, half), f32),
            pltpu.VMEM(near_trig.shape, f32),
            pltpu.VMEM(far_trig.shape[1:], f32),
            pltpu.SemaphoreType.DMA((5,)),
            pltpu.VMEM((count, LANES), f32),
            pltpu.VMEM((count, LANES), f32),
            pltpu.VMEM((QUERY_BLOCK, QUERY_BLOCK), bf16),
            pltpu.VMEM((QUERY_BLOCK, QUERY_BLOCK), bf16),
            pltpu.VMEM(row_data.shape, bf16),
            pltpu.VMEM(query_weight.shape, bf16),
            pltpu.VMEM((key_weight.shape[0], 2 * key_weight.shape[1]), bf16),
            pltpu.VMEM(out_weight.shape, bf16),
            pltpu.SemaphoreType.DMA((2,)),
            pltpu.SemaphoreType.DMA((3,)),
            pltpu.VMEM((count // KEY_BLOCK, KEY_BLOCK, 2 * LANES), bf16),
            pltpu.VMEM((devices * qblocks, KEY_BLOCK, 2 * LANES), bf16),
            pltpu.VMEM((devices * qblocks, KEY_BLOCK, 2 * LANES), bf16),
            pltpu.VMEM((count, heads_width), bf16),
            pltpu.VMEM((LANES + QUERY_BLOCK, 2 * key_count), bf16),
            pltpu.VMEM((2 * key_count, 2 * LANES), bf16),
            pltpu.VMEM((heads_width // LANES * QUERY_BLOCK, 2 * key_count), f32),
            pltpu.VMEM((heads_width // LANES * QUERY_BLOCK, 2 * key_count), bf16),
            pltpu.VMEM((count, heads_width), bf16),
            pltpu.VMEM((count, heads_width), bf16),
            pltpu.VMEM((QUERY_BLOCK, 2 * half), bf16),
            pltpu.VMEM((count, half), f32),
            pltpu.VMEM((qblocks - 2, QUERY_BLOCK, LANES), f32),
            pltpu.VMEM((qblocks - 2, QUERY_BLOCK, LANES), f32),
            pltpu.SemaphoreType.DMA((devices,)),
            pltpu.SemaphoreType.DMA((qblocks + 1,)),
            pltpu.SemaphoreType.DMA((2,)),
            pltpu.SemaphoreType.DMA((1,)),
            pltpu.SemaphoreType.DMA((count // ROWS + 1,)),
            pltpu.SemaphoreType.DMA((1,)),
            pltpu.SemaphoreType.DMA((count // ROWS - 1,)),
        ],
        compiler_params=pltpu.CompilerParams(
            collective_id=0, has_side_effects=True, vmem_limit_bytes=48 * 1024 * 1024
        ),
    )(*operands)
    result = [pltpu.with_memory_space_constraint(x, pltpu.VMEM) for x in result]
    return pl.pallas_call(
        finish_kernel,
        out_shape=jax.ShapeDtypeStruct((count, half), bf16),
        in_specs=[vmem] * len(result),
        out_specs=hbm,
        scratch_shapes=[
            pltpu.VMEM((QUERY_BLOCK, half), f32),
            pltpu.VMEM((QUERY_BLOCK, half), bf16),
            pltpu.SemaphoreType.DMA((2,)),
        ],
        compiler_params=pltpu.CompilerParams(vmem_limit_bytes=8 * 1024 * 1024),
    )(*result)[None]


def solution(mesh):
    placed = (
        P("dp", "kv", None),
        P(None, "tp"),
        P(None, "tp"),
        P(None, "tp"),
        P("tp", None),
        P("tp"),
        P("dp", None, None),
        P("dp", None, None),
    )
    return jax.shard_map(
        body, mesh=mesh, in_specs=placed, out_specs=P("dp", "kv", "tp"), check_vma=False
    )
```

```python
import functools

import jax
import jax.numpy as jnp
import numpy as np
from jax import lax
from jax.experimental import pallas as pl
from jax.experimental.pallas import tpu as pltpu
from jax.sharding import PartitionSpec as P

HEAD_DIM = 64
QUERY_BLOCK = 128
KEY_BLOCK = 64
LANES = 128
ROWS = 256
COLS = 256

rope_base = 10000.0
norm_eps = 1e-06
hidden = -1e38
MESH = pl.DeviceIdType.MESH


def low_lanes(shape):
    return lax.broadcasted_iota(jnp.int32, shape, 1) < HEAD_DIM


def turn(u, cosine, sine):
    lane = lax.broadcasted_iota(jnp.int32, u.shape, 1)
    half = HEAD_DIM // 2
    swapped = jnp.where(
        lane % HEAD_DIM < half, pltpu.roll(u, LANES - half, 1), pltpu.roll(u, half, 1)
    )
    return u * cosine + swapped * sine


def part_of(left, right, rows, half, side, c):
    cols = pl.ds(pl.multiple_of(side * half + c * COLS, COLS), COLS)
    return jnp.dot(
        left[rows, :], right[:, cols], preferred_element_type=jnp.float32
    ).astype(jnp.bfloat16)


def squares(total, added):
    for k in range(COLS // LANES):
        piece = added[:, k * LANES : (k + 1) * LANES]
        total = total + piece * piece
    return total


def row_scale(total, half):
    return lax.rsqrt(jnp.sum(total, axis=1, keepdims=True) / (2 * half) + norm_eps)


def kernel(
    devices, owner_hbm, part_hbm, tok_hbm, wq_hbm, wk_hbm, wv_hbm, ow_hbm, gain_hbm, near_hbm, far_hbm, out, mix_end, ow_other, partial, gain_end,
    owner_ref, part_ref, gain, near_trig, far_trig, small_sems, cosine, sine, eye, causal,
    tok, wq, wkv, ow, tok_sems, weight_sems,
    kv, send, pool, queries, keys_now, values_now, scores, weights, mix, mix_other, early, proj,
    kv_send, kv_recv, ow_sems, mix_send, mix_recv,
):
    me = lax.axis_index("kv")
    core = lax.axis_index("tp")
    other = 1 - core
    tokens = tok.shape[0]
    qblocks = tokens // QUERY_BLOCK
    chosen = owner_ref.shape[0]
    half = gain.shape[1]
    row_steps = tokens // ROWS
    per_q = QUERY_BLOCK // KEY_BLOCK
    key_width = wk_hbm.shape[1]
    slices = wq.shape[1] // LANES
    heads = wq.shape[1] // HEAD_DIM
    bf16, f32 = jnp.bfloat16, jnp.float32

    pieces = ((0, ROWS), (ROWS, tokens - ROWS))

    def tok_copy(r):
        rows = pl.ds(*pieces[r])
        return pltpu.make_async_copy(tok_hbm.at[rows], tok.at[rows], tok_sems.at[r])

    wk_copy = pltpu.make_async_copy(wk_hbm, wkv.at[:, pl.ds(0, key_width)], weight_sems.at[0])
    wv_copy = pltpu.make_async_copy(
        wv_hbm, wkv.at[:, pl.ds(key_width, key_width)], weight_sems.at[0]
    )
    wq_copy = pltpu.make_async_copy(wq_hbm, wq, weight_sems.at[1])
    ow_loads = []
    for m in range(slices):
        for g in range(2):
            ow_loads.append(
                pltpu.make_async_copy(
                    ow_hbm.at[pl.ds((g * slices + m) * HEAD_DIM, HEAD_DIM)],
                    ow.at[pl.ds((2 * m + g) * HEAD_DIM, HEAD_DIM)],
                    weight_sems.at[2],
                )
            )
    small = [
        pltpu.make_async_copy(near_hbm, near_trig, small_sems.at[0]),
        pltpu.make_async_copy(far_hbm.at[me], far_trig, small_sems.at[4]),
        pltpu.make_async_copy(owner_hbm, owner_ref, small_sems.at[1]),
        pltpu.make_async_copy(part_hbm, part_ref, small_sems.at[2]),
        pltpu.make_async_copy(gain_hbm, gain, small_sems.at[3]),
    ]
    small[0].start()
    small[1].start()
    wk_copy.start()
    wv_copy.start()
    tok_copy(0).start()
    tok_copy(1).start(priority=1)
    for copy in small[2:]:
        copy.start(priority=1)

    barrier = pltpu.get_barrier_semaphore()

    @pl.loop(0, devices)
    def _(j):
        @pl.when(j != me)
        def _():
            pl.semaphore_signal(barrier, inc=1, device_id={"kv": j}, device_id_type=MESH)

    pl.semaphore_signal(barrier, inc=1, device_id={"tp": other}, device_id_type=MESH)

    square = (QUERY_BLOCK, QUERY_BLOCK)
    first = lax.broadcasted_iota(jnp.int32, square, 0)
    second = lax.broadcasted_iota(jnp.int32, square, 1)
    eye[...] = jnp.where(first == second, 1.0, 0.0).astype(bf16)
    causal[...] = jnp.where(first >= second, 0.0, hidden).astype(bf16)

    small[0].wait()
    small[1].wait()
    near_cos = near_trig[0:QUERY_BLOCK, :]
    near_sin = near_trig[QUERY_BLOCK : 2 * QUERY_BLOCK, :]

    @pl.loop(0, qblocks)
    def _(b):
        rows = pl.ds(pl.multiple_of(b * QUERY_BLOCK, QUERY_BLOCK), QUERY_BLOCK)
        far_cos = far_trig[pl.ds(b, 1), :]
        far_sin = far_trig[pl.ds(b + qblocks, 1), :]
        cosine[rows, :] = far_cos * near_cos - far_sin * near_sin
        sine[rows, :] = far_sin * near_cos + far_cos * near_sin

    pltpu.make_async_copy(wkv, wkv, weight_sems.at[0]).wait()

    once = jnp.where(core >= 0, 1, 0)
    for r, (start, size) in enumerate(pieces):

        @pl.loop(0, once)
        def _(_):
            tok_copy(r).wait()
            if r == 0:
                wq_copy.start(priority=1)
                for copy in ow_loads:
                    copy.start(priority=1)
            rows = pl.ds(start, size)
            both = jnp.dot(tok[rows, :], wkv[...], preferred_element_type=f32)
            keys = turn(both[:, :LANES], cosine[rows, :], sine[rows, :])
            joined = jnp.concatenate([keys, both[:, LANES:]], axis=1).astype(bf16)
            blocks = size // KEY_BLOCK
            kv[pl.ds(start // KEY_BLOCK, blocks)] = joined.reshape(blocks, KEY_BLOCK, 2 * LANES)

    for copy in small[2:]:
        copy.wait()
    pl.semaphore_wait(barrier, devices)

    def place(src, row, s):
        return owner_ref[s, row] == src, part_ref[s, row]

    def wanted(dst, q):
        found = [place(me, dst * qblocks + q, s) for s in range(chosen)]
        return sum(jnp.where(here, at, 0) for here, at in found)

    def kv_copy(dst, q, lanes, sem):
        return pltpu.make_async_remote_copy(
            src_ref=send.at[pl.ds(dst * qblocks + q, 1), :, lanes],
            dst_ref=pool.at[pl.ds(q * devices + me, 1), :, lanes],
            send_sem=kv_send.at[0],
            recv_sem=kv_recv.at[sem],
            device_id={"kv": dst},
            device_id_type=MESH,
        )

    last = qblocks - 1
    all_lanes, key_lanes, value_lanes = (
        pl.ds(0, 2 * LANES), pl.ds(0, LANES), pl.ds(LANES, LANES)
    )

    paced = me + 3 < devices

    def send_block(q, split):
        @pl.loop(0, devices - 1)
        def _(step):
            dst = jnp.where(paced, step + 1, devices - 1 - step)

            @pl.when(dst > me)
            def _():
                send[pl.ds(dst * qblocks + q, 1)] = kv[pl.ds(wanted(dst, q), 1)]
                kv_copy(dst, q, key_lanes if split else all_lanes, q).start()

        if split:

            @pl.loop(1, devices)
            def _(dst):
                @pl.when(dst > me)
                def _():
                    kv_copy(dst, q, value_lanes, qblocks).start()

    @pl.loop(0, jnp.where(paced, 1, last))
    def _(q):
        send_block(q, False)

    @pl.when(jnp.logical_not(paced))
    def _():
        send_block(last, True)

    @pl.loop(0, qblocks)
    def _(q):
        pool[pl.ds(q * devices + me, 1)] = kv[pl.ds(wanted(me, q), 1)]

        @pl.loop(0, devices)
        def _(src):
            @pl.when(src > me)
            def _():
                pool[pl.ds(q * devices + src, 1)] = jnp.zeros((1, KEY_BLOCK, 2 * LANES), bf16)

    ow_copy = pltpu.make_async_remote_copy(
        src_ref=ow,
        dst_ref=ow_other,
        send_sem=ow_sems.at[0],
        recv_sem=ow_sems.at[1],
        device_id={"tp": other},
        device_id_type=MESH,
    )
    wq_copy.wait()

    @pl.loop(0, row_steps)
    def _(r):
        @pl.when(jnp.logical_and(paced, r == row_steps - 1))
        def _():
            send_block(1, False)

        @pl.when(r == 1)
        def _():
            pltpu.make_async_copy(ow, ow, weight_sems.at[2]).wait()
            ow_copy.start()

        rows = pl.ds(pl.multiple_of(r * ROWS, ROWS), ROWS)
        scale = HEAD_DIM**-0.5
        scaled_cos, scaled_sin = cosine[rows, :] * scale, sine[rows, :] * scale
        for c in range(wq.shape[1] // COLS):
            part = jnp.dot(
                tok[rows, :], wq[:, c * COLS : (c + 1) * COLS], preferred_element_type=f32
            )
            for k in range(COLS // LANES):
                turned = turn(part[:, k * LANES : (k + 1) * LANES], scaled_cos, scaled_sin)
                away = pltpu.roll(turned, HEAD_DIM, 1)
                for j in range(2):
                    head = 2 * (c * (COLS // LANES) + k) + j
                    group, m = head // slices, head % slices
                    lanes = slice(group * HEAD_DIM, (group + 1) * HEAD_DIM)
                    at = m * LANES + group * HEAD_DIM
                    queries[rows, at : at + HEAD_DIM] = (
                        turned if group == j else away
                    )[:, lanes].astype(bf16)

    key_count = devices * KEY_BLOCK + QUERY_BLOCK

    blocks_in = ROWS // QUERY_BLOCK

    def group_of(b):
        return b // blocks_in + jnp.where(b == last, 1, 0)

    def wait_mix(first, count):
        rows = pl.ds(pl.multiple_of(first * QUERY_BLOCK, QUERY_BLOCK), count * QUERY_BLOCK)
        landed = mix_other.at[rows]
        pltpu.make_async_copy(landed, landed, mix_recv.at[group_of(first)]).wait()

    def mix_copy(b):
        rows = pl.ds(pl.multiple_of(b * QUERY_BLOCK, QUERY_BLOCK), QUERY_BLOCK)
        return pltpu.make_async_remote_copy(
            src_ref=mix.at[rows],
            dst_ref=mix_other.at[rows] if b is not last else mix_end,
            send_sem=mix_send.at[0],
            recv_sem=mix_recv.at[group_of(b)],
            device_id={"tp": other},
            device_id_type=MESH,
        )

    low_mask = jnp.where(low_lanes((key_count, LANES)), 1.0, 0.0).astype(bf16)
    high_mask = jnp.where(low_lanes((key_count, LANES)), 0.0, 1.0).astype(bf16)

    def wait_kv(b, lanes, sem):
        for n in range(1, devices):

            @pl.when(me == n)
            def _():
                landed = pool.at[pl.ds(b * devices, n), :, lanes]
                pltpu.make_async_copy(landed, landed, kv_recv.at[sem]).wait()

    def block_of(b, lanes):
        far = pool[pl.ds(b * devices, devices), :, lanes].reshape(devices * KEY_BLOCK, LANES)
        near = kv[pl.ds(b * per_q, per_q), :, lanes].reshape(QUERY_BLOCK, LANES)
        return jnp.concatenate([far, near], axis=0)

    sections = [slice(m * QUERY_BLOCK, (m + 1) * QUERY_BLOCK) for m in range(slices)]

    def attend_keys(b):
        row = me * qblocks + b
        rows = pl.ds(pl.multiple_of(b * QUERY_BLOCK, QUERY_BLOCK), QUERY_BLOCK)
        keys = block_of(b, slice(0, LANES))
        owner = lax.broadcasted_iota(jnp.int32, (1, devices * KEY_BLOCK), 1) // KEY_BLOCK
        bias = jnp.full((1, devices * KEY_BLOCK), hidden, f32)
        for s in range(chosen):
            bias = jnp.where(owner == owner_ref[s, row], 0.0, bias)
        bias = jnp.broadcast_to(bias, (QUERY_BLOCK, devices * KEY_BLOCK)).astype(bf16)
        bias = jnp.concatenate([bias, causal[...]], axis=1)
        turned = keys.T
        blank = jnp.zeros((HEAD_DIM, key_count), bf16)
        wide_keys = jnp.concatenate(
            [
                jnp.concatenate([turned[:HEAD_DIM], blank, bias], axis=0),
                jnp.concatenate([blank, turned[HEAD_DIM:], bias], axis=0),
            ],
            axis=1,
        )
        keys_now[...] = wide_keys
        for m, section in enumerate(sections):
            q = jnp.concatenate([queries[rows, m * LANES : (m + 1) * LANES], eye[...]], axis=1)
            scores[section, :] = jnp.dot(q, keys_now[...], preferred_element_type=f32)
        for section in sections:
            for side in range(2):
                cols = slice(side * key_count, (side + 1) * key_count)
                s = scores[section, cols]
                weights[section, cols] = jnp.exp(s - jnp.max(s, axis=1, keepdims=True)).astype(bf16)

    def attend_values(b):
        rows = pl.ds(pl.multiple_of(b * QUERY_BLOCK, QUERY_BLOCK), QUERY_BLOCK)
        values = block_of(b, slice(LANES, 2 * LANES))
        values_now[...] = jnp.concatenate(
            [
                jnp.concatenate([values * low_mask, low_mask], axis=1),
                jnp.concatenate([values * high_mask, high_mask], axis=1),
            ],
            axis=0,
        )
        for m, section in enumerate(sections):
            mixed = jnp.dot(weights[section, :], values_now[...], preferred_element_type=f32)
            mix[rows, m * LANES : (m + 1) * LANES] = (mixed[:, :LANES] / mixed[:, LANES:]).astype(
                bf16
            )
        mix_copy(b).start()

    def project_mine(first, count, held):
        size = count * QUERY_BLOCK
        rows = pl.ds(pl.multiple_of(first * QUERY_BLOCK, QUERY_BLOCK), size)
        for n, side in enumerate((other, core)):
            for c in range(half // COLS):
                at = n * half + c * COLS
                held[:size, at : at + COLS] = part_of(mix, ow, rows, half, side, c)

    def project_theirs(first, count):
        wait_mix(first, count)
        size = count * QUERY_BLOCK
        rows = pl.ds(pl.multiple_of(first * QUERY_BLOCK, QUERY_BLOCK), size)
        total = jnp.zeros((size, LANES), f32)
        for n, side in enumerate((other, core)):
            for c in range(half // COLS):
                at = n * half + c * COLS
                theirs = part_of(mix_other, ow_other, rows, half, side, c)
                added = early[:size, at : at + COLS].astype(f32) + theirs.astype(f32)
                if side is core:
                    proj[:size, c * COLS : (c + 1) * COLS] = added
                total = squares(total, added)
        scale = row_scale(total, half)
        for c in range(half // LANES):
            at = slice(c * LANES, (c + 1) * LANES)
            out[rows, at] = (proj[:size, at] * scale * gain[:, at]).astype(bf16)

    @pl.loop(0, last)
    def _(b):
        wait_kv(b, all_lanes, b)
        attend_keys(b)
        attend_values(b)

        @pl.when(b == 1)
        def _():
            ow_copy.wait_recv()

        @pl.when(jnp.logical_and(paced, jnp.logical_and(b > 0, b < last - 2)))
        def _():
            send_block(b + 1, False)

        @pl.when(b % blocks_in == blocks_in - 1)
        def _():
            project_mine(b + 1 - blocks_in, blocks_in, early)
            project_theirs(b + 1 - blocks_in, blocks_in)

        @pl.when(jnp.logical_and(paced, b == last - 2))
        def _():
            send_block(last - 1, False)

    @pl.when(paced)
    def _():
        send_block(last, True)

    project_mine(last - 1, 1, early)
    gain_end[...] = gain[...]
    wait_kv(last, key_lanes, last)
    attend_keys(last)
    wait_kv(last, value_lanes, qblocks)
    attend_values(last)
    project_mine(last, 1, partial)
    project_theirs(last - 1, 1)

    for n in range(devices - 1):

        @pl.when(me == n)
        def _():
            sent = send.at[pl.ds((n + 1) * qblocks, (devices - 1 - n) * qblocks)]
            pltpu.make_async_copy(sent, sent, kv_send.at[0]).wait()

    ow_copy.wait_send()
    pltpu.make_async_copy(mix_end, mix_end, mix_recv.at[group_of(last)]).wait()
    pltpu.make_async_copy(mix, mix, mix_send.at[0]).wait()


def finish_kernel(held, mix_end, ow_other, partial, gain, out, proj, end, sems):
    core = lax.axis_index("tp")
    half = gain.shape[1]
    early = held.shape[0] - QUERY_BLOCK
    rows = pl.ds(0, early)
    first = pltpu.make_async_copy(held.at[rows], out.at[rows], sems.at[0])
    first.start()
    every = slice(0, QUERY_BLOCK)
    total = jnp.zeros((QUERY_BLOCK, LANES), jnp.float32)
    for n, side in enumerate((1 - core, core)):
        for c in range(half // COLS):
            at = n * half + c * COLS
            theirs = part_of(mix_end, ow_other, every, half, side, c)
            mine = partial[:, at : at + COLS]
            added = mine.astype(jnp.float32) + theirs.astype(jnp.float32)
            if side is core:
                proj[:, c * COLS : (c + 1) * COLS] = added
            total = squares(total, added)
    scale = row_scale(total, half)
    for c in range(half // LANES):
        at = slice(c * LANES, (c + 1) * LANES)
        end[:, at] = (proj[:, at] * scale * gain[:, at]).astype(jnp.bfloat16)
    final = pltpu.make_async_copy(end, out.at[pl.ds(early, QUERY_BLOCK)], sems.at[1])
    final.start()
    first.wait()
    final.wait()


def trig_table(devices, blocks):
    half_dim = HEAD_DIM // 2
    lane = np.arange(LANES)
    frequency = (rope_base ** (-(lane % half_dim) / half_dim)).astype(np.float32)
    sign = np.where(lane % HEAD_DIM < half_dim, -1.0, 1.0)
    near = np.arange(QUERY_BLOCK)[:, None] * frequency.astype(np.float64)
    far = (np.arange(blocks)[:, None] * np.float32(QUERY_BLOCK) * frequency).astype(np.float64)
    near = np.concatenate([np.cos(near), sign * np.sin(near)], axis=0)
    far = np.stack([np.cos(far), sign * np.sin(far)]).reshape(2, devices, -1, LANES)
    far = far.transpose(1, 0, 2, 3).reshape(devices, -1, LANES)
    return near.astype(np.float32), far.astype(np.float32)


def body(
    tokens, query_weight, key_weight, value_weight, out_weight, norm_gain, chosen_owner, chosen_part
):
    row_data = tokens[0]
    count = row_data.shape[0]
    devices = lax.axis_size("kv")
    qblocks = count // QUERY_BLOCK
    heads_width = query_weight.shape[1]
    half = norm_gain.shape[0]
    hbm = pl.BlockSpec(memory_space=pl.ANY)
    vmem = pl.BlockSpec(memory_space=pltpu.VMEM)
    bf16, f32 = jnp.bfloat16, jnp.float32
    slots = chosen_owner.shape[1:][::-1]
    key_count = devices * KEY_BLOCK + QUERY_BLOCK
    near_trig, far_trig = trig_table(devices, devices * qblocks)
    operands = [
        chosen_owner[0].T, chosen_part[0].T, row_data, query_weight, key_weight, value_weight,
        out_weight, norm_gain[None], jnp.asarray(near_trig), jnp.asarray(far_trig),
    ]
    operands = [pltpu.with_memory_space_constraint(x, pltpu.HBM) for x in operands]
    result = pl.pallas_call(
        functools.partial(kernel, devices),
        out_shape=[
            pltpu.VMEM((count, half), bf16),
            pltpu.VMEM((QUERY_BLOCK, heads_width), bf16),
            pltpu.VMEM(out_weight.shape, bf16),
            pltpu.VMEM((QUERY_BLOCK, 2 * half), bf16),
            pltpu.VMEM((1, half), f32),
        ],
        in_specs=[hbm] * len(operands),
        out_specs=[vmem] * 5,
        scratch_shapes=[
            pltpu.SMEM(slots, jnp.int32),
            pltpu.SMEM(slots, jnp.int32),
            pltpu.VMEM((1, half), f32),
            pltpu.VMEM(near_trig.shape, f32),
            pltpu.VMEM(far_trig.shape[1:], f32),
            pltpu.SemaphoreType.DMA((5,)),
            pltpu.VMEM((count, LANES), f32),
            pltpu.VMEM((count, LANES), f32),
            pltpu.VMEM((QUERY_BLOCK, QUERY_BLOCK), bf16),
            pltpu.VMEM((QUERY_BLOCK, QUERY_BLOCK), bf16),
            pltpu.VMEM(row_data.shape, bf16),
            pltpu.VMEM(query_weight.shape, bf16),
            pltpu.VMEM((key_weight.shape[0], 2 * key_weight.shape[1]), bf16),
            pltpu.VMEM(out_weight.shape, bf16),
            pltpu.SemaphoreType.DMA((2,)),
            pltpu.SemaphoreType.DMA((3,)),
            pltpu.VMEM((count // KEY_BLOCK, KEY_BLOCK, 2 * LANES), bf16),
            pltpu.VMEM((devices * qblocks, KEY_BLOCK, 2 * LANES), bf16),
            pltpu.VMEM((devices * qblocks, KEY_BLOCK, 2 * LANES), bf16),
            pltpu.VMEM((count, heads_width), bf16),
            pltpu.VMEM((LANES + QUERY_BLOCK, 2 * key_count), bf16),
            pltpu.VMEM((2 * key_count, 2 * LANES), bf16),
            pltpu.VMEM((heads_width // LANES * QUERY_BLOCK, 2 * key_count), f32),
            pltpu.VMEM((heads_width // LANES * QUERY_BLOCK, 2 * key_count), bf16),
            pltpu.VMEM((count, heads_width), bf16),
            pltpu.VMEM((count, heads_width), bf16),
            pltpu.VMEM((ROWS, 2 * half), bf16),
            pltpu.VMEM((ROWS, half), f32),
            pltpu.SemaphoreType.DMA((1,)),
            pltpu.SemaphoreType.DMA((qblocks + 1,)),
            pltpu.SemaphoreType.DMA((2,)),
            pltpu.SemaphoreType.DMA((1,)),
            pltpu.SemaphoreType.DMA((count // ROWS + 1,)),
        ],
        compiler_params=pltpu.CompilerParams(
            collective_id=0, has_side_effects=True, vmem_limit_bytes=48 * 1024 * 1024
        ),
    )(*operands)
    result = [pltpu.with_memory_space_constraint(x, pltpu.VMEM) for x in result]
    return pl.pallas_call(
        finish_kernel,
        out_shape=jax.ShapeDtypeStruct((count, half), bf16),
        in_specs=[vmem] * len(result),
        out_specs=hbm,
        scratch_shapes=[
            pltpu.VMEM((QUERY_BLOCK, half), f32),
            pltpu.VMEM((QUERY_BLOCK, half), bf16),
            pltpu.SemaphoreType.DMA((2,)),
        ],
        compiler_params=pltpu.CompilerParams(vmem_limit_bytes=8 * 1024 * 1024),
    )(*result)[None]


def solution(mesh):
    placed = (
        P("dp", "kv", None),
        P(None, "tp"),
        P(None, "tp"),
        P(None, "tp"),
        P("tp", None),
        P("tp"),
        P("dp", None, None),
        P("dp", None, None),
    )
    return jax.shard_map(
        body, mesh=mesh, in_specs=placed, out_specs=P("dp", "kv", "tp"), check_vma=False
    )
```

```python
import functools

import jax
import jax.numpy as jnp
import numpy as np
from jax import lax
from jax.experimental import pallas as pl
from jax.experimental.pallas import tpu as pltpu
from jax.sharding import PartitionSpec as P

HEAD_DIM = 64
QUERY_BLOCK = 128
KEY_BLOCK = 64
LANES = 128
ROWS = 256
COLS = 256

rope_base = 10000.0
norm_eps = 1e-06
hidden = -1e38
MESH = pl.DeviceIdType.MESH


def low_lanes(shape):
    return lax.broadcasted_iota(jnp.int32, shape, 1) < HEAD_DIM


def turn(u, cosine, sine):
    lane = lax.broadcasted_iota(jnp.int32, u.shape, 1)
    half = HEAD_DIM // 2
    swapped = jnp.where(
        lane % HEAD_DIM < half, pltpu.roll(u, LANES - half, 1), pltpu.roll(u, half, 1)
    )
    return u * cosine + swapped * sine


def part_of(left, right, rows, half, side, c):
    cols = pl.ds(pl.multiple_of(side * half + c * COLS, COLS), COLS)
    return jnp.dot(
        left[rows, :], right[:, cols], preferred_element_type=jnp.float32
    ).astype(jnp.bfloat16)


def squares(total, added):
    for k in range(COLS // LANES):
        piece = added[:, k * LANES : (k + 1) * LANES]
        total = total + piece * piece
    return total


def row_scale(total, half):
    return lax.rsqrt(jnp.sum(total, axis=1, keepdims=True) / (2 * half) + norm_eps)


def kernel(
    devices, owner_hbm, part_hbm, tok_hbm, wq_hbm, wk_hbm, wv_hbm, ow_hbm, gain_hbm, near_hbm, far_hbm, out, mix_end, ow_other, partial, gain_end,
    owner_ref, part_ref, gain, near_trig, far_trig, small_sems, cosine, sine, eye, causal,
    tok, wq, wkv, ow, tok_sems, weight_sems,
    kv, send, pool, queries, keys_now, values_now, scores, weights, mix, mix_other, early, proj,
    kv_send, kv_recv, ow_sems, mix_send, mix_recv,
):
    me = lax.axis_index("kv")
    core = lax.axis_index("tp")
    other = 1 - core
    tokens = tok.shape[0]
    qblocks = tokens // QUERY_BLOCK
    chosen = owner_ref.shape[0]
    half = gain.shape[1]
    row_steps = tokens // ROWS
    per_q = QUERY_BLOCK // KEY_BLOCK
    key_width = wk_hbm.shape[1]
    slices = wq.shape[1] // LANES
    heads = wq.shape[1] // HEAD_DIM
    bf16, f32 = jnp.bfloat16, jnp.float32

    first_rows = tokens // KEY_BLOCK * 5 // 12 * KEY_BLOCK
    pieces = ((0, first_rows), (first_rows, tokens - first_rows))

    def tok_copy(r):
        rows = pl.ds(*pieces[r])
        return pltpu.make_async_copy(tok_hbm.at[rows], tok.at[rows], tok_sems.at[r])

    wk_copy = pltpu.make_async_copy(wk_hbm, wkv.at[:, pl.ds(0, key_width)], weight_sems.at[0])
    wv_copy = pltpu.make_async_copy(
        wv_hbm, wkv.at[:, pl.ds(key_width, key_width)], weight_sems.at[0]
    )
    wq_copy = pltpu.make_async_copy(wq_hbm, wq, weight_sems.at[1])
    ow_loads = []
    for m in range(slices):
        for g in range(2):
            ow_loads.append(
                pltpu.make_async_copy(
                    ow_hbm.at[pl.ds((g * slices + m) * HEAD_DIM, HEAD_DIM)],
                    ow.at[pl.ds((2 * m + g) * HEAD_DIM, HEAD_DIM)],
                    weight_sems.at[2],
                )
            )
    small = [
        pltpu.make_async_copy(near_hbm, near_trig, small_sems.at[0]),
        pltpu.make_async_copy(far_hbm.at[me], far_trig, small_sems.at[4]),
        pltpu.make_async_copy(owner_hbm, owner_ref, small_sems.at[1]),
        pltpu.make_async_copy(part_hbm, part_ref, small_sems.at[2]),
        pltpu.make_async_copy(gain_hbm, gain, small_sems.at[3]),
    ]
    small[0].start()
    small[1].start()
    wk_copy.start()
    wv_copy.start()
    tok_copy(0).start()
    tok_copy(1).start(priority=1)
    for copy in small[2:]:
        copy.start(priority=1)

    barrier = pltpu.get_barrier_semaphore()

    @pl.loop(0, devices)
    def _(j):
        @pl.when(j != me)
        def _():
            pl.semaphore_signal(barrier, inc=1, device_id={"kv": j}, device_id_type=MESH)

    pl.semaphore_signal(barrier, inc=1, device_id={"tp": other}, device_id_type=MESH)

    square = (QUERY_BLOCK, QUERY_BLOCK)
    first = lax.broadcasted_iota(jnp.int32, square, 0)
    second = lax.broadcasted_iota(jnp.int32, square, 1)
    eye[...] = jnp.where(first == second, 1.0, 0.0).astype(bf16)
    causal[...] = jnp.where(first >= second, 0.0, hidden).astype(bf16)

    small[0].wait()
    small[1].wait()
    near_cos = near_trig[0:QUERY_BLOCK, :]
    near_sin = near_trig[QUERY_BLOCK : 2 * QUERY_BLOCK, :]

    @pl.loop(0, qblocks)
    def _(b):
        rows = pl.ds(pl.multiple_of(b * QUERY_BLOCK, QUERY_BLOCK), QUERY_BLOCK)
        far_cos = far_trig[pl.ds(b, 1), :]
        far_sin = far_trig[pl.ds(b + qblocks, 1), :]
        cosine[rows, :] = far_cos * near_cos - far_sin * near_sin
        sine[rows, :] = far_sin * near_cos + far_cos * near_sin

    pltpu.make_async_copy(wkv, wkv, weight_sems.at[0]).wait()

    once = jnp.where(core >= 0, 1, 0)
    for r, (start, size) in enumerate(pieces):

        @pl.loop(0, once)
        def _(_):
            tok_copy(r).wait()
            if r == 0:
                wq_copy.start(priority=1)
                for copy in ow_loads:
                    copy.start(priority=1)
            rows = pl.ds(start, size)
            both = jnp.dot(tok[rows, :], wkv[...], preferred_element_type=f32)
            keys = turn(both[:, :LANES], cosine[rows, :], sine[rows, :])
            joined = jnp.concatenate([keys, both[:, LANES:]], axis=1).astype(bf16)
            blocks = size // KEY_BLOCK
            kv[pl.ds(start // KEY_BLOCK, blocks)] = joined.reshape(blocks, KEY_BLOCK, 2 * LANES)

    for copy in small[2:]:
        copy.wait()
    pl.semaphore_wait(barrier, devices)

    def place(src, row, s):
        return owner_ref[s, row] == src, part_ref[s, row]

    def wanted(dst, q):
        found = [place(me, dst * qblocks + q, s) for s in range(chosen)]
        return sum(jnp.where(here, at, 0) for here, at in found)

    def kv_copy(dst, q, lanes, sem):
        return pltpu.make_async_remote_copy(
            src_ref=send.at[pl.ds(dst * qblocks + q, 1), :, lanes],
            dst_ref=pool.at[pl.ds(q * devices + me, 1), :, lanes],
            send_sem=kv_send.at[0],
            recv_sem=kv_recv.at[sem],
            device_id={"kv": dst},
            device_id_type=MESH,
        )

    last = qblocks - 1
    all_lanes, key_lanes, value_lanes = (
        pl.ds(0, 2 * LANES), pl.ds(0, LANES), pl.ds(LANES, LANES)
    )

    paced = me + 3 < devices

    def send_block(q, split):
        @pl.loop(0, devices - 1)
        def _(step):
            dst = devices - 1 - step

            @pl.when(dst > me)
            def _():
                send[pl.ds(dst * qblocks + q, 1)] = kv[pl.ds(wanted(dst, q), 1)]
                kv_copy(dst, q, key_lanes if split else all_lanes, q).start()

        if split:

            @pl.loop(1, devices)
            def _(dst):
                @pl.when(dst > me)
                def _():
                    kv_copy(dst, q, value_lanes, qblocks).start()

    @pl.loop(0, jnp.where(paced, 1, last))
    def _(q):
        send_block(q, False)

    @pl.when(jnp.logical_not(paced))
    def _():
        send_block(last, True)

    @pl.loop(0, qblocks)
    def _(q):
        pool[pl.ds(q * devices + me, 1)] = kv[pl.ds(wanted(me, q), 1)]

        @pl.loop(0, devices)
        def _(src):
            @pl.when(src > me)
            def _():
                pool[pl.ds(q * devices + src, 1)] = jnp.zeros((1, KEY_BLOCK, 2 * LANES), bf16)

    ow_copy = pltpu.make_async_remote_copy(
        src_ref=ow,
        dst_ref=ow_other,
        send_sem=ow_sems.at[0],
        recv_sem=ow_sems.at[1],
        device_id={"tp": other},
        device_id_type=MESH,
    )
    wq_copy.wait()

    @pl.loop(0, row_steps)
    def _(r):
        @pl.when(jnp.logical_and(paced, r == row_steps - 1))
        def _():
            send_block(1, False)

        @pl.when(r == 1)
        def _():
            pltpu.make_async_copy(ow, ow, weight_sems.at[2]).wait()
            ow_copy.start()

        rows = pl.ds(pl.multiple_of(r * ROWS, ROWS), ROWS)
        scale = HEAD_DIM**-0.5
        scaled_cos, scaled_sin = cosine[rows, :] * scale, sine[rows, :] * scale
        for c in range(wq.shape[1] // COLS):
            part = jnp.dot(
                tok[rows, :], wq[:, c * COLS : (c + 1) * COLS], preferred_element_type=f32
            )
            for k in range(COLS // LANES):
                turned = turn(part[:, k * LANES : (k + 1) * LANES], scaled_cos, scaled_sin)
                away = pltpu.roll(turned, HEAD_DIM, 1)
                for j in range(2):
                    head = 2 * (c * (COLS // LANES) + k) + j
                    group, m = head // slices, head % slices
                    lanes = slice(group * HEAD_DIM, (group + 1) * HEAD_DIM)
                    at = m * LANES + group * HEAD_DIM
                    queries[rows, at : at + HEAD_DIM] = (
                        turned if group == j else away
                    )[:, lanes].astype(bf16)

    key_count = devices * KEY_BLOCK + QUERY_BLOCK

    blocks_in = ROWS // QUERY_BLOCK

    def group_of(b):
        return b // blocks_in + jnp.where(b == last, 1, 0)

    def wait_mix(first, count):
        rows = pl.ds(pl.multiple_of(first * QUERY_BLOCK, QUERY_BLOCK), count * QUERY_BLOCK)
        landed = mix_other.at[rows]
        pltpu.make_async_copy(landed, landed, mix_recv.at[group_of(first)]).wait()

    def mix_copy(b):
        rows = pl.ds(pl.multiple_of(b * QUERY_BLOCK, QUERY_BLOCK), QUERY_BLOCK)
        return pltpu.make_async_remote_copy(
            src_ref=mix.at[rows],
            dst_ref=mix_other.at[rows] if b is not last else mix_end,
            send_sem=mix_send.at[0],
            recv_sem=mix_recv.at[group_of(b)],
            device_id={"tp": other},
            device_id_type=MESH,
        )

    low_mask = jnp.where(low_lanes((key_count, LANES)), 1.0, 0.0).astype(bf16)
    high_mask = jnp.where(low_lanes((key_count, LANES)), 0.0, 1.0).astype(bf16)

    def wait_kv(b, lanes, sem):
        for n in range(1, devices):

            @pl.when(me == n)
            def _():
                landed = pool.at[pl.ds(b * devices, n), :, lanes]
                pltpu.make_async_copy(landed, landed, kv_recv.at[sem]).wait()

    def block_of(b, lanes):
        far = pool[pl.ds(b * devices, devices), :, lanes].reshape(devices * KEY_BLOCK, LANES)
        near = kv[pl.ds(b * per_q, per_q), :, lanes].reshape(QUERY_BLOCK, LANES)
        return jnp.concatenate([far, near], axis=0)

    sections = [slice(m * QUERY_BLOCK, (m + 1) * QUERY_BLOCK) for m in range(slices)]

    def attend_keys(b):
        row = me * qblocks + b
        rows = pl.ds(pl.multiple_of(b * QUERY_BLOCK, QUERY_BLOCK), QUERY_BLOCK)
        keys = block_of(b, slice(0, LANES))
        owner = lax.broadcasted_iota(jnp.int32, (1, devices * KEY_BLOCK), 1) // KEY_BLOCK
        bias = jnp.full((1, devices * KEY_BLOCK), hidden, f32)
        for s in range(chosen):
            bias = jnp.where(owner == owner_ref[s, row], 0.0, bias)
        bias = jnp.broadcast_to(bias, (QUERY_BLOCK, devices * KEY_BLOCK)).astype(bf16)
        bias = jnp.concatenate([bias, causal[...]], axis=1)
        turned = keys.T
        blank = jnp.zeros((HEAD_DIM, key_count), bf16)
        wide_keys = jnp.concatenate(
            [
                jnp.concatenate([turned[:HEAD_DIM], blank, bias], axis=0),
                jnp.concatenate([blank, turned[HEAD_DIM:], bias], axis=0),
            ],
            axis=1,
        )
        keys_now[...] = wide_keys
        for m, section in enumerate(sections):
            q = jnp.concatenate([queries[rows, m * LANES : (m + 1) * LANES], eye[...]], axis=1)
            scores[section, :] = jnp.dot(q, keys_now[...], preferred_element_type=f32)
        for section in sections:
            for side in range(2):
                cols = slice(side * key_count, (side + 1) * key_count)
                s = scores[section, cols]
                weights[section, cols] = jnp.exp(s - jnp.max(s, axis=1, keepdims=True)).astype(bf16)

    def attend_values(b):
        rows = pl.ds(pl.multiple_of(b * QUERY_BLOCK, QUERY_BLOCK), QUERY_BLOCK)
        values = block_of(b, slice(LANES, 2 * LANES))
        values_now[...] = jnp.concatenate(
            [
                jnp.concatenate([values * low_mask, low_mask], axis=1),
                jnp.concatenate([values * high_mask, high_mask], axis=1),
            ],
            axis=0,
        )
        for m, section in enumerate(sections):
            mixed = jnp.dot(weights[section, :], values_now[...], preferred_element_type=f32)
            mix[rows, m * LANES : (m + 1) * LANES] = (mixed[:, :LANES] / mixed[:, LANES:]).astype(
                bf16
            )
        mix_copy(b).start()

    def project_mine(first, count, held):
        size = count * QUERY_BLOCK
        rows = pl.ds(pl.multiple_of(first * QUERY_BLOCK, QUERY_BLOCK), size)
        for n, side in enumerate((other, core)):
            for c in range(half // COLS):
                at = n * half + c * COLS
                held[:size, at : at + COLS] = part_of(mix, ow, rows, half, side, c)

    def project_theirs(first, count):
        wait_mix(first, count)
        size = count * QUERY_BLOCK
        rows = pl.ds(pl.multiple_of(first * QUERY_BLOCK, QUERY_BLOCK), size)
        total = jnp.zeros((size, LANES), f32)
        for n, side in enumerate((other, core)):
            for c in range(half // COLS):
                at = n * half + c * COLS
                theirs = part_of(mix_other, ow_other, rows, half, side, c)
                added = early[:size, at : at + COLS].astype(f32) + theirs.astype(f32)
                if side is core:
                    proj[:size, c * COLS : (c + 1) * COLS] = added
                total = squares(total, added)
        scale = row_scale(total, half)
        for c in range(half // LANES):
            at = slice(c * LANES, (c + 1) * LANES)
            out[rows, at] = (proj[:size, at] * scale * gain[:, at]).astype(bf16)

    @pl.loop(0, last)
    def _(b):
        wait_kv(b, all_lanes, b)
        attend_keys(b)
        attend_values(b)

        @pl.when(b == 1)
        def _():
            ow_copy.wait_recv()

        @pl.when(jnp.logical_and(paced, jnp.logical_and(b > 0, b < last - 2)))
        def _():
            send_block(b + 1, False)

        @pl.when(b % blocks_in == blocks_in - 1)
        def _():
            project_mine(b + 1 - blocks_in, blocks_in, early)
            project_theirs(b + 1 - blocks_in, blocks_in)

        @pl.when(jnp.logical_and(paced, b == last - 2))
        def _():
            send_block(last - 1, False)

    @pl.when(paced)
    def _():
        send_block(last, True)

    project_mine(last - 1, 1, early)
    gain_end[...] = gain[...]
    wait_kv(last, key_lanes, last)
    attend_keys(last)
    wait_kv(last, value_lanes, qblocks)
    attend_values(last)
    project_mine(last, 1, partial)
    project_theirs(last - 1, 1)

    for n in range(devices - 1):

        @pl.when(me == n)
        def _():
            sent = send.at[pl.ds((n + 1) * qblocks, (devices - 1 - n) * qblocks)]
            pltpu.make_async_copy(sent, sent, kv_send.at[0]).wait()

    ow_copy.wait_send()
    pltpu.make_async_copy(mix_end, mix_end, mix_recv.at[group_of(last)]).wait()
    pltpu.make_async_copy(mix, mix, mix_send.at[0]).wait()


def finish_kernel(held, mix_end, ow_other, partial, gain, out, proj, end, sems):
    core = lax.axis_index("tp")
    half = gain.shape[1]
    early = held.shape[0] - QUERY_BLOCK
    rows = pl.ds(0, early)
    first = pltpu.make_async_copy(held.at[rows], out.at[rows], sems.at[0])
    first.start()
    every = slice(0, QUERY_BLOCK)
    total = jnp.zeros((QUERY_BLOCK, LANES), jnp.float32)
    for n, side in enumerate((1 - core, core)):
        for c in range(half // COLS):
            at = n * half + c * COLS
            theirs = part_of(mix_end, ow_other, every, half, side, c)
            mine = partial[:, at : at + COLS]
            added = mine.astype(jnp.float32) + theirs.astype(jnp.float32)
            if side is core:
                proj[:, c * COLS : (c + 1) * COLS] = added
            total = squares(total, added)
    scale = row_scale(total, half)
    for c in range(half // LANES):
        at = slice(c * LANES, (c + 1) * LANES)
        end[:, at] = (proj[:, at] * scale * gain[:, at]).astype(jnp.bfloat16)
    final = pltpu.make_async_copy(end, out.at[pl.ds(early, QUERY_BLOCK)], sems.at[1])
    final.start()
    first.wait()
    final.wait()


def trig_table(devices, blocks):
    half_dim = HEAD_DIM // 2
    lane = np.arange(LANES)
    frequency = (rope_base ** (-(lane % half_dim) / half_dim)).astype(np.float32)
    sign = np.where(lane % HEAD_DIM < half_dim, -1.0, 1.0)
    near = np.arange(QUERY_BLOCK)[:, None] * frequency.astype(np.float64)
    far = (np.arange(blocks)[:, None] * np.float32(QUERY_BLOCK) * frequency).astype(np.float64)
    near = np.concatenate([np.cos(near), sign * np.sin(near)], axis=0)
    far = np.stack([np.cos(far), sign * np.sin(far)]).reshape(2, devices, -1, LANES)
    far = far.transpose(1, 0, 2, 3).reshape(devices, -1, LANES)
    return near.astype(np.float32), far.astype(np.float32)


def body(
    tokens, query_weight, key_weight, value_weight, out_weight, norm_gain, chosen_owner, chosen_part
):
    row_data = tokens[0]
    count = row_data.shape[0]
    devices = lax.axis_size("kv")
    qblocks = count // QUERY_BLOCK
    heads_width = query_weight.shape[1]
    half = norm_gain.shape[0]
    hbm = pl.BlockSpec(memory_space=pl.ANY)
    vmem = pl.BlockSpec(memory_space=pltpu.VMEM)
    bf16, f32 = jnp.bfloat16, jnp.float32
    slots = chosen_owner.shape[1:][::-1]
    key_count = devices * KEY_BLOCK + QUERY_BLOCK
    near_trig, far_trig = trig_table(devices, devices * qblocks)
    operands = [
        chosen_owner[0].T, chosen_part[0].T, row_data, query_weight, key_weight, value_weight,
        out_weight, norm_gain[None], jnp.asarray(near_trig), jnp.asarray(far_trig),
    ]
    operands = [pltpu.with_memory_space_constraint(x, pltpu.HBM) for x in operands]
    result = pl.pallas_call(
        functools.partial(kernel, devices),
        out_shape=[
            pltpu.VMEM((count, half), bf16),
            pltpu.VMEM((QUERY_BLOCK, heads_width), bf16),
            pltpu.VMEM(out_weight.shape, bf16),
            pltpu.VMEM((QUERY_BLOCK, 2 * half), bf16),
            pltpu.VMEM((1, half), f32),
        ],
        in_specs=[hbm] * len(operands),
        out_specs=[vmem] * 5,
        scratch_shapes=[
            pltpu.SMEM(slots, jnp.int32),
            pltpu.SMEM(slots, jnp.int32),
            pltpu.VMEM((1, half), f32),
            pltpu.VMEM(near_trig.shape, f32),
            pltpu.VMEM(far_trig.shape[1:], f32),
            pltpu.SemaphoreType.DMA((5,)),
            pltpu.VMEM((count, LANES), f32),
            pltpu.VMEM((count, LANES), f32),
            pltpu.VMEM((QUERY_BLOCK, QUERY_BLOCK), bf16),
            pltpu.VMEM((QUERY_BLOCK, QUERY_BLOCK), bf16),
            pltpu.VMEM(row_data.shape, bf16),
            pltpu.VMEM(query_weight.shape, bf16),
            pltpu.VMEM((key_weight.shape[0], 2 * key_weight.shape[1]), bf16),
            pltpu.VMEM(out_weight.shape, bf16),
            pltpu.SemaphoreType.DMA((2,)),
            pltpu.SemaphoreType.DMA((3,)),
            pltpu.VMEM((count // KEY_BLOCK, KEY_BLOCK, 2 * LANES), bf16),
            pltpu.VMEM((devices * qblocks, KEY_BLOCK, 2 * LANES), bf16),
            pltpu.VMEM((devices * qblocks, KEY_BLOCK, 2 * LANES), bf16),
            pltpu.VMEM((count, heads_width), bf16),
            pltpu.VMEM((LANES + QUERY_BLOCK, 2 * key_count), bf16),
            pltpu.VMEM((2 * key_count, 2 * LANES), bf16),
            pltpu.VMEM((heads_width // LANES * QUERY_BLOCK, 2 * key_count), f32),
            pltpu.VMEM((heads_width // LANES * QUERY_BLOCK, 2 * key_count), bf16),
            pltpu.VMEM((count, heads_width), bf16),
            pltpu.VMEM((count, heads_width), bf16),
            pltpu.VMEM((ROWS, 2 * half), bf16),
            pltpu.VMEM((ROWS, half), f32),
            pltpu.SemaphoreType.DMA((1,)),
            pltpu.SemaphoreType.DMA((qblocks + 1,)),
            pltpu.SemaphoreType.DMA((2,)),
            pltpu.SemaphoreType.DMA((1,)),
            pltpu.SemaphoreType.DMA((count // ROWS + 1,)),
        ],
        compiler_params=pltpu.CompilerParams(
            collective_id=0, has_side_effects=True, vmem_limit_bytes=48 * 1024 * 1024
        ),
    )(*operands)
    result = [pltpu.with_memory_space_constraint(x, pltpu.VMEM) for x in result]
    return pl.pallas_call(
        finish_kernel,
        out_shape=jax.ShapeDtypeStruct((count, half), bf16),
        in_specs=[vmem] * len(result),
        out_specs=hbm,
        scratch_shapes=[
            pltpu.VMEM((QUERY_BLOCK, half), f32),
            pltpu.VMEM((QUERY_BLOCK, half), bf16),
            pltpu.SemaphoreType.DMA((2,)),
        ],
        compiler_params=pltpu.CompilerParams(vmem_limit_bytes=8 * 1024 * 1024),
    )(*result)[None]


def solution(mesh):
    placed = (
        P("dp", "kv", None),
        P(None, "tp"),
        P(None, "tp"),
        P(None, "tp"),
        P("tp", None),
        P("tp"),
        P("dp", None, None),
        P("dp", None, None),
    )
    return jax.shard_map(
        body, mesh=mesh, in_specs=placed, out_specs=P("dp", "kv", "tp"), check_vma=False
    )
```
